32 devices in a mesh: ep: 8 (over z, x), tp: 4 (over y, core).
Axes of the slice: x: 2, y: 2, z: 4, core: 2. Of those that a mesh axis runs over, the one named last changes fastest.
Arguments:
- first_batch: bfloat16 [4096, 2048], P(('ep', 'tp')), may hold values from -6 to 6
- mixer_gain: float32 [2048], replicated, may hold values from 0.1 to 1.9
- mixer_in: bfloat16 [2048, 512], P(None, 'tp'), may hold values from -0.125 to 0.125
- group_maps: bfloat16 [8, 64, 64], replicated, may hold values from -0.75 to 0.75
- pool_scale: float32 [512], replicated, may hold values from 0.1 to 1.9
- mixer_out: bfloat16 [512, 2048], P('tp'), may hold values from -0.25 to 0.25
- second_batch: bfloat16 [1024, 2048], P('ep'), may hold values from -6 to 6
- expert_gain: float32 [2048], replicated, may hold values from 0.1 to 1.9
- expert_choice: int32 [1024, 2], P('ep'), may hold values from 0 to 7, all different within a row; in each aligned block of 128 rows (0 to 127, 128 to 255, ...) at most 64 rows name the same one
- route_scores: float32 [1024, 2], P('ep'), may hold values from -6 to 6
- expert_gate: bfloat16 [8, 2048, 3584], P('ep', None, 'tp'), may hold values from -0.125 to 0.125
- expert_up: bfloat16 [8, 2048, 3584], P('ep', None, 'tp'), may hold values from -0.125 to 0.125
- expert_down: bfloat16 [8, 3584, 2048], P('ep', 'tp'), may hold values from -0.09375 to 0.09375
Outputs:
- mixed_first: bfloat16 [4096, 2048], P(('ep', 'tp'))
- experts_second: bfloat16 [1024, 2048], P('ep')
The draws below stay inside these ranges and needn't reach their ends.
Inputs may be any that keep to these rules, and one draw needn't show every extreme that they name: `expert_choice`: the two entries of a row differ. Within the rows of one device (aligned blocks of 128 rows) no expert is named more than 64 times, a bound that some block reaches there.
All inputs are finite; a program needn't handle non-finite values.
Results may differ from the reference program's by a relative error of at most 0.018.
Values may be sent and summed in bfloat16 or wider, within the bound.
A program may use at most 64 MiB of HBM per device.

```python
import math
import jax
import jax.numpy as jnp
import numpy as np
from jax import lax

D = 2048
POOL = 512
GROUP = 64
FF_E = 3584
TOP = 2
SEQS = 1
ROWS_B = 128
EXPERTS = 8
CAP = 64
GROUPS = 8
TOKENS_A = 4096
TOKENS_B = 1024
N_TP = 4


def block_scale(rng, extent, shards, smallest, largest):
    def one(dim, parts):
        steps = jax.random.uniform(jax.random.fold_in(jax.random.fold_in(rng, 6), dim), (parts,), jnp.float32, smallest / len(shards), largest / len(shards))
        return jnp.repeat(jnp.exp(steps), extent[dim] // parts).reshape((-1,) + (1,) * (len(extent) - dim - 1))

    level = one(*shards[0])
    for cut in shards[1:]:
        level = level * one(*cut)
    return level


def shared_out(key, own, number, rows, number_of, top, bound, skew):
    sequence = jax.random.permutation(key, number_of)
    packed, common = load_shares(number_of, rows * top, bound, skew, True), load_shares(number_of, rows * top, bound, skew, False)
    places = jnp.arange(number_of)

    def named(lengths, offset_by):
        used = int((lengths > 0).sum())
        fixed = max(1, used // 4)
        moved = fixed + (places - fixed + offset_by * (used - fixed)) % max(1, number_of - fixed)
        return jnp.zeros((number_of,), jnp.int32).at[sequence[jnp.where(places < fixed, places, moved)]].set(jnp.asarray(lengths, jnp.int32))

    lengths = jnp.where(number % 4 == 0, named(packed, number // 4), named(common, number - number // 4 - 1))
    mixed = jax.random.permutation(jax.random.fold_in(own, 3), number_of)
    source_of, receiver = mixed[0:number_of // 2 * 2:2], mixed[1:number_of // 2 * 2:2]
    room = jnp.minimum(lengths[source_of] - 1, bound - lengths[receiver]) // 2
    room = jnp.where((source_of == sequence[0]) | (receiver == sequence[0]) | (lengths[receiver] == 0), 0, jnp.maximum(room, 0))
    moved = jax.random.randint(jax.random.fold_in(own, 4), (number_of // 2,), 0, 1 << 20) % (room + 1)
    lengths = lengths.at[source_of].add(-moved).at[receiver].add(moved)
    members = jnp.searchsorted(jnp.cumsum(lengths), jnp.arange(rows * top), side="right").astype(jnp.int32)
    grid = members.reshape(top, rows).T
    grid = grid[jax.random.permutation(jax.random.fold_in(own, 1), rows)]
    offset_by = jax.random.randint(jax.random.fold_in(own, 2), (rows, 1), 0, top)
    return jnp.take_along_axis(grid, (jnp.arange(top)[None, :] + offset_by) % top, axis=1)


def load_shares(count, total, most, lean, full):
    portions = [(1 << 20) // math.isqrt(standing ** lean) + 1 for standing in range(1, count + 1)]
    largest = most if full else min(most, max(-(-total // count), total * portions[0] // sum(portions)))
    least = 1 if total - largest >= count - 1 else 0
    counts, rest = [largest] + [least] * (count - 1), total - largest - least * (count - 1)
    while rest > 0:
        free = [i for i in range(1, count) if counts[i] < largest] or [i for i in range(1, count) if counts[i] < most]
        whole, left = sum([portions[i] for i in free]), rest
        for i in free:
            extra = min(most - counts[i], max(1, left * portions[i] // whole), rest)
            counts[i] = counts[i] + extra
            rest = rest - extra
    return np.array(counts)


def noise(rng, dims, width, limit, split=(), held_as=jnp.bfloat16):
    loudness = block_scale(rng, dims, split, -0.22, 0.18) if split else 1.0
    array = jax.random.normal(rng, dims, jnp.float32) * width * loudness
    return jnp.minimum(jnp.maximum(array, -limit), limit).astype(held_as)


def setup_inputs(seed: int = 0) -> dict:
    keys = jax.random.split(jax.random.key(seed), 14)
    first_batch = noise(keys[0], (TOKENS_A, D), 1.0, 6.0, ((0, 32),))
    mixer_gain = jnp.clip(1.0 + 0.18 * jax.random.normal(keys[1], (D,), jnp.float32), 0.1, 1.9)
    mixer_in = noise(keys[2], (D, POOL), D ** -0.5, 0.125, ((1, 4),))
    group_maps = noise(keys[3], (GROUPS, GROUP, GROUP), GROUP ** -0.5, 0.75)
    pool_scale = jnp.clip(1.0 + 0.18 * jax.random.normal(keys[4], (POOL,), jnp.float32), 0.1, 1.9)
    mixer_out = noise(keys[5], (POOL, D), POOL ** -0.5, 0.25, ((0, 4),))
    second_batch = noise(keys[6], (TOKENS_B, D), 1.0, 6.0, ((0, 8),))
    expert_gain = jnp.clip(1.0 + 0.18 * jax.random.normal(keys[7], (D,), jnp.float32), 0.1, 1.9)
    expert_choice_keys = jax.random.split(jax.random.fold_in(keys[8], 1), TOKENS_B // ROWS_B)
    expert_choice_turns = jax.random.permutation(jax.random.fold_in(keys[8], 3), TOKENS_B // ROWS_B)
    expert_choice = jax.vmap(lambda own, number: shared_out(jax.random.fold_in(keys[8], 2), own, number, ROWS_B, EXPERTS, TOP, CAP, 1))(expert_choice_keys, expert_choice_turns).reshape((TOKENS_B, TOP))
    route_scores = noise(keys[9], (TOKENS_B, TOP), 1.5, 6.0, ((0, 8),), jnp.float32)
    expert_gate = noise(keys[10], (EXPERTS, D, FF_E), D ** -0.5, 0.125, ((0, 8), (2, 4)))
    expert_up = noise(keys[11], (EXPERTS, D, FF_E), D ** -0.5, 0.125, ((0, 8), (2, 4)))
    expert_down = noise(keys[12], (EXPERTS, FF_E, D), FF_E ** -0.5, 0.09375, ((0, 8), (1, 4)))
    return dict(first_batch=first_batch, mixer_gain=mixer_gain, mixer_in=mixer_in, group_maps=group_maps, pool_scale=pool_scale, mixer_out=mixer_out, second_batch=second_batch, expert_gain=expert_gain, expert_choice=expert_choice, route_scores=route_scores, expert_gate=expert_gate, expert_up=expert_up, expert_down=expert_down)


windows = (2, 4, 8, 16)
epsilon = 1e-06

def rms_scale(values, gain):
    floats = values.astype(jnp.float32)
    factor = lax.rsqrt(lax.optimization_barrier(jnp.mean(floats * floats, axis=-1, keepdims=True)) + epsilon)
    return (floats * factor * gain).astype(jnp.bfloat16)

def pool_centred(pooled_in):
    total = pooled_in.shape[0]
    seq_length = total // SEQS
    pooled_f32 = pooled_in.astype(jnp.float32).reshape(SEQS, seq_length, POOL)
    running = jnp.pad(jnp.cumsum(pooled_f32, axis=1), ((0, 0), (1, 0), (0, 0)))
    places = jnp.arange(seq_length, dtype=jnp.int32)
    pieces = []
    for group in range(POOL // GROUP):
        half_span = windows[group % 4] // 2
        upper_end = jnp.clip(places + half_span, 0, seq_length)
        lower_end = jnp.clip(places - half_span, 0, seq_length)
        group_sums = running[:, :, group * GROUP:(group + 1) * GROUP]
        window_sum = jnp.take(group_sums, upper_end, axis=1) - jnp.take(group_sums, lower_end, axis=1)
        window_count = (upper_end - lower_end).astype(jnp.float32)[None, :, None]
        pieces.append(window_sum / window_count - pooled_f32[:, :, group * GROUP:(group + 1) * GROUP])
    return jnp.concatenate(pieces, axis=-1).reshape(total, POOL).astype(jnp.bfloat16)

def reference(first_batch, mixer_gain, mixer_in, group_maps, pool_scale, mixer_out, second_batch, expert_gain, expert_choice, route_scores, expert_gate, expert_up, expert_down):
    normed_first = rms_scale(first_batch, mixer_gain)
    pooled_in = jnp.dot(normed_first, mixer_in, preferred_element_type=jnp.float32).astype(jnp.bfloat16)
    centred = pool_centred(pooled_in)
    group_count = POOL // GROUP
    grouped = jnp.einsum('tgc,gcd->tgd', centred.reshape(-1, group_count, GROUP).astype(jnp.float32), group_maps.astype(jnp.float32))
    grouped = (grouped.reshape(-1, POOL) * pool_scale).astype(jnp.bfloat16)
    mixed_first = jnp.dot(grouped, mixer_out, preferred_element_type=jnp.float32).astype(jnp.bfloat16)
    expert_count = expert_gate.shape[0]
    block_count = second_batch.shape[0] // ROWS_B
    normed_second = rms_scale(second_batch, expert_gain)
    chosen = expert_choice.reshape(block_count, ROWS_B * TOP)
    one_hot = (chosen[:, :, None] == jnp.arange(expert_count, dtype=jnp.int32)[None, None, :]).astype(jnp.int32)
    ranking = lax.optimization_barrier(jnp.sum(jnp.cumsum(one_hot, axis=1) * one_hot, axis=2)) - 1
    local_rows = jnp.arange(ROWS_B * TOP, dtype=jnp.int32) // TOP
    global_rows = local_rows[None, :] + (jnp.arange(block_count, dtype=jnp.int32) * ROWS_B)[:, None]
    block_index = jnp.arange(block_count, dtype=jnp.int32)[:, None]
    slot_place = ((chosen * block_count + block_index) * CAP + ranking).reshape(-1)
    slot_table = jnp.zeros((expert_count * block_count * CAP,), jnp.int32).at[slot_place].set(global_rows.reshape(-1) + 1)
    slot_table = slot_table.reshape(expert_count, block_count * CAP)
    split_size = FF_E // N_TP

    def one_expert(operands):
        row_index, gate_weight, up_weight, down_weight = operands
        live_rows = row_index > 0
        taken = jnp.where(live_rows[:, None], normed_second[jnp.maximum(row_index - 1, 0)], jnp.zeros((), jnp.bfloat16))
        gate_part = jnp.dot(taken, gate_weight, preferred_element_type=jnp.float32)
        up_part = jnp.dot(taken, up_weight, preferred_element_type=jnp.float32)
        hidden = (jax.nn.silu(gate_part) * up_part).astype(jnp.bfloat16)
        partial_value = jnp.einsum('rtf,tfd->trd', hidden.reshape(-1, N_TP, split_size).astype(jnp.float32), down_weight.reshape(N_TP, split_size, D).astype(jnp.float32))
        rounded = lax.optimization_barrier(partial_value.astype(jnp.bfloat16))
        return lax.optimization_barrier(jnp.sum(rounded.astype(jnp.float32), axis=0)).astype(jnp.bfloat16)
    results = lax.map(one_expert, (slot_table, expert_gate, expert_up, expert_down))
    flat_results = results.reshape(expert_count * block_count * CAP, D)
    picked = flat_results[slot_place].reshape(-1, TOP, D).astype(jnp.float32)
    weight_first = jax.nn.sigmoid(route_scores[:, 0] - route_scores[:, 1])[:, None]
    experts_second = (weight_first * picked[:, 0] + (1.0 - weight_first) * picked[:, 1]).astype(jnp.bfloat16)
    return (mixed_first, experts_second)
```

```python
import jax
import jax.numpy as jnp
from jax import lax
from jax.experimental import pallas as pl
from jax.experimental.pallas import tpu as pltpu
from jax.sharding import PartitionSpec as P

GROUP = 64
SEQS = 1


epsilon = 1e-06


def extended(block, sides, width):
    for axis, dim in sides:
        count = lax.axis_size(axis)
        forward = [(i, i + 1) for i in range(count - 1)]
        backward = [(target, source) for source, target in forward]
        low = lax.ppermute(
            lax.slice_in_dim(block, block.shape[dim] - width, None, axis=dim), axis, forward
        )
        high = lax.ppermute(lax.slice_in_dim(block, 0, width, axis=dim), axis, backward)
        block = jnp.concatenate([low, block, high], axis=dim)
    return block


def rms_scale(values, gain):
    floats = values.astype(jnp.float32)
    factor = lax.rsqrt(jnp.mean(floats * floats, axis=-1, keepdims=True) + epsilon)
    return (floats * factor * gain).astype(jnp.bfloat16)


def mixer_half(first_batch, mixer_gain, mixer_in, group_maps, pool_scale, mixer_out):
    count_rows = first_batch.shape[0]
    normed = rms_scale(first_batch, mixer_gain)
    pooled_in = jnp.dot(
        normed,
        lax.all_gather(mixer_in, "tp", axis=1, tiled=True),
        preferred_element_type=jnp.float32,
    ).astype(jnp.bfloat16)
    channels = pooled_in.shape[1]
    padded = extended(pooled_in, ((("ep", "tp"), 0),), 8).astype(jnp.float32)
    devices = lax.axis_size("ep") * lax.axis_size("tp")
    seq_length = count_rows * devices // SEQS
    first_row = (lax.axis_index("ep") * lax.axis_size("tp") + lax.axis_index("tp")) * count_rows
    places = first_row + jnp.arange(count_rows, dtype=jnp.int32)
    own_seq = places // seq_length
    group_of = jnp.arange(channels, dtype=jnp.int32) // GROUP
    half_span = jnp.left_shift(jnp.ones_like(group_of), group_of % 4)
    window_sum = jnp.zeros((count_rows, channels), jnp.float32)
    window_count = jnp.zeros((count_rows, channels), jnp.float32)
    for offset in range(-8, 8):
        inside = (
            ((places + offset) // seq_length == own_seq)[:, None]
            & (offset >= -half_span)[None, :]
            & (offset < half_span)[None, :]
        )
        window_sum = window_sum + jnp.where(
            inside, padded[8 + offset : 8 + offset + count_rows], 0.0
        )
        window_count = window_count + inside.astype(jnp.float32)
    centred = (window_sum / window_count - padded[8 : 8 + count_rows]).astype(jnp.bfloat16)
    group_count = group_maps.shape[0]
    identity = jnp.eye(group_count, dtype=jnp.bfloat16)
    block_map = jnp.einsum("gcd,gh->gchd", group_maps, identity).reshape(channels, channels)
    grouped = (jnp.dot(centred, block_map, preferred_element_type=jnp.float32) * pool_scale).astype(
        jnp.bfloat16
    )
    mixed_out = jnp.dot(
        grouped,
        lax.all_gather(mixer_out, "tp", axis=0, tiled=True),
        preferred_element_type=jnp.float32,
    )
    return mixed_out.astype(jnp.bfloat16)


def expert_half(
    second_batch, expert_gain, expert_choice, route_scores, expert_gate, expert_up, expert_down
):
    row_count = second_batch.shape[0]
    model_width = second_batch.shape[1]
    experts = lax.axis_size("ep")
    tp_count = lax.axis_size("tp")
    capacity = 4 * row_count // experts
    share = capacity // tp_count
    normed = rms_scale(second_batch, expert_gain)
    chosen = expert_choice.reshape(-1)
    one_hot = (chosen[:, None] == jnp.arange(experts, dtype=jnp.int32)[None, :]).astype(jnp.int32)
    ranking = jnp.sum(jnp.cumsum(one_hot, axis=0) * one_hot, axis=1) - 1
    slot_place = ranking * experts + chosen
    source_row = jnp.arange(chosen.shape[0], dtype=jnp.int32) // expert_choice.shape[1]
    slot_table = jnp.zeros((capacity * experts,), jnp.int32).at[slot_place].set(source_row + 1)
    outgoing = jnp.where(
        (slot_table > 0)[:, None],
        normed[jnp.maximum(slot_table - 1, 0)],
        jnp.zeros((), jnp.bfloat16),
    )
    outgoing = outgoing.reshape(capacity, experts, model_width)
    portion = lax.dynamic_slice_in_dim(outgoing, lax.axis_index("tp") * share, share, 0)
    arrived_part = lax.all_to_all(portion, "ep", split_axis=1, concat_axis=1, tiled=True)
    arrived = lax.all_gather(arrived_part, "tp", axis=0, tiled=True)
    incoming = arrived.reshape(capacity * experts, model_width)
    gate_weight = expert_gate[0]
    up_weight = expert_up[0]
    down_weight = expert_down[0]
    gate_part = jnp.dot(incoming, gate_weight, preferred_element_type=jnp.float32)
    up_part = jnp.dot(incoming, up_weight, preferred_element_type=jnp.float32)
    hidden = (jax.nn.silu(gate_part) * up_part).astype(jnp.bfloat16)
    summed = lax.psum_scatter(
        jnp.dot(hidden, down_weight, preferred_element_type=jnp.float32).astype(jnp.bfloat16),
        "tp",
        scatter_dimension=0,
        tiled=True,
    )
    finished = summed.reshape(share, experts, model_width)
    returned = lax.all_to_all(finished, "ep", split_axis=1, concat_axis=1, tiled=True)
    every_slot = lax.all_gather(returned, "tp", axis=0, tiled=True).reshape(
        capacity * experts, model_width
    )
    picked = every_slot[slot_place].reshape(row_count, -1, model_width)
    weight_first = jax.nn.sigmoid(route_scores[:, 0] - route_scores[:, 1])[:, None]
    blended = weight_first * picked[:, 0].astype(jnp.float32) + (1.0 - weight_first) * picked[
        :, 1
    ].astype(jnp.float32)
    return blended.astype(jnp.bfloat16)


MESH = pl.DeviceIdType.MESH
VMEM_LIMIT = 60 * 1024 * 1024
F32 = jnp.float32
BF16 = jnp.bfloat16


def flip(row, relation):
    place = row
    for bit in (1, 2, 4):
        if relation & bit:
            place = place + bit * (1 - 2 * ((row // bit) % 2))
    return place


def weave(main, extra):
    taken = 0
    for i, step in enumerate(main):
        step()
        due = (i + 1) * len(extra) // len(main)
        while taken < due:
            extra[taken]()
            taken += 1


def normalize(source, gain, target):
    for i in range(0, source.shape[0], 16):
        floats = source[i : i + 16].astype(F32)
        factor = lax.rsqrt(jnp.mean(floats * floats, axis=-1, keepdims=True) + epsilon)
        target[i : i + 16] = (floats * factor * gain[...]).astype(BF16)


def layer_kernel(
    first_hbm, mixer_gain_hbm, mixer_in_hbm, maps_hbm, scale_hbm, mixer_out_hbm,
    second_hbm, expert_gain_hbm, choice_hbm, scores_hbm, gate_hbm, up_hbm, down_hbm,
    mixed_hbm, result_hbm,
    x1, x2, n1, n2, gain1, gain2, scale, choice, scores, maps,
    w_in, w_down, m1, m2,
    rank_of, pick, portion, landed, hidden, part,
    side_y, side_own, sums_y, from_y, sums, slots, high, low, pieces,
    padded, floats, grouped, mixed,
    load, d_send, d_recv, c_send, c_recv, m_send, m_recv, h_send, h_recv, f_send, f_recv, store,
):
    row, col = lax.axis_index("ep"), lax.axis_index("tp")
    count = landed.shape[0]
    share = landed.shape[2]
    capacity = 4 * share
    rows, width = x2.shape
    quarter = width // 4
    tiles = w_in.shape[0]
    shard = m1.shape[1] // 4
    partner = col + 1 - 2 * (col % 2)
    across = (col + 2) % 4
    corner = (partner + 2) % 4
    devices = 4 * count
    index = row * 4 + col
    after, before = (index + 1) % devices, (index + devices - 1) % devices
    after_device, before_device = (after // 4, after % 4), (before // 4, before % 4)
    peer = [(flip(row, k), col) for k in range(count)]
    on_chip, over_y = (row, partner), (row, across)

    def remote(source, target, send, recv, device):
        return pltpu.make_async_remote_copy(
            src_ref=source, dst_ref=target, send_sem=send, recv_sem=recv,
            device_id=device, device_id_type=MESH,
        )

    def shard_of(which):
        return pl.ds(pl.multiple_of(which * shard, shard), shard)

    loads = {}

    def fetch(name, source, target):
        loads[name] = pltpu.make_async_copy(source, target, load.at[len(loads)])
        loads[name].start()

    fetch("x2", second_hbm, x2)
    fetch("gain2", expert_gain_hbm, gain2)
    fetch("choice", choice_hbm, choice)
    fetch("scores", scores_hbm, scores)
    fetch("m1", mixer_in_hbm, m1.at[:, shard_of(col)])
    fetch("m2", mixer_out_hbm, m2.at[shard_of(col)])
    fetch("x1", first_hbm, x1)
    fetch("gain1", mixer_gain_hbm, gain1)
    fetch("maps", maps_hbm, maps)
    fetch("scale", scale_hbm, scale)
    for j in range(tiles):
        fetch(f"gate{j}", gate_hbm.at[0, :, pl.ds(128 * j, 128)], w_in.at[j, :, pl.ds(0, 128)])
        fetch(f"up{j}", up_hbm.at[0, :, pl.ds(128 * j, 128)], w_in.at[j, :, pl.ds(128, 128)])
    fetch("down", down_hbm.at[0], w_down)

    barrier = pltpu.get_barrier_semaphore()
    peers = peer[1:] + [on_chip, over_y, after_device, before_device]
    for device in peers:
        pl.semaphore_signal(barrier, inc=1, device_id=device, device_id_type=MESH)

    loads["choice"].wait()
    experts = lax.broadcasted_iota(jnp.int32, (16, rows), 0)
    first, second = choice[0:1], choice[1:2]
    named = (first == experts) | (second == experts)
    earlier = lax.broadcasted_iota(jnp.int32, (rows, rows), 0) < lax.broadcasted_iota(
        jnp.int32, (rows, rows), 1
    )
    rank = jnp.dot(
        named.astype(F32).astype(BF16), earlier.astype(F32).astype(BF16), preferred_element_type=F32
    )
    rank_of[...] = jnp.where(named, rank, -1.0)

    def rank_at(k):
        return rank_of[pl.ds(peer[k][0], 1), :]

    place = lax.broadcasted_iota(jnp.int32, (capacity, rows), 0).astype(F32)
    offset = (col * share).astype(F32)
    for k in range(1, count):
        chosen = place[:share] + offset == rank_at(k)
        pick[(k - 1) * share : k * share] = chosen.astype(F32).astype(BF16)
    own = (count - 1) * share
    pick[own:] = (place == rank_at(0)).astype(F32).astype(BF16)

    loads["x2"].wait()
    loads["gain2"].wait()
    normalize(x2, gain2, n2)
    for n in range(0, width, 256):
        taken = jnp.dot(pick[...], n2[:, n : n + 256], preferred_element_type=F32).astype(BF16)
        portion[:, :, n : n + 256] = taken[:own].reshape(count - 1, share, 256)
        landed[0, :, :, n : n + 256] = taken[own:].reshape(4, share, 256)

    loads["m1"].wait()
    loads["m2"].wait()
    pl.semaphore_wait(barrier, len(peers))

    firsts, ys, sides, corners = {}, {}, {}, {}
    for k in FIRST_ORDER:
        firsts[k] = remote(
            portion.at[k - 1], landed.at[k, col], d_send.at[0, k], d_recv.at[0, k], peer[k]
        )
        firsts[k].start()

    def forward(k):
        def run():
            firsts[k].wait_recv()
            block = landed.at[k, col]
            ys[k] = remote(block, block, d_send.at[1, k], d_recv.at[1, k], over_y)
            ys[k].start()
            sides[k] = remote(block, block, d_send.at[2, k], d_recv.at[2, k], on_chip)
            sides[k].start()

        return run

    def turn(k):
        def run():
            ys[k].wait_recv()
            block = landed.at[k, across]
            corners[k] = remote(block, block, d_send.at[3, k], d_recv.at[3, k], on_chip)
            corners[k].start()

        return run

    fourth = row % 4
    moves = []

    def piece(which, owner, start, size):
        if which == 0:
            unit = m1.shape[0] // 4
            return m1.at[pl.ds(pl.multiple_of(start * unit, unit), size * unit), shard_of(owner)]
        unit = shard // 4
        return m2.at[pl.ds(pl.multiple_of(owner * shard + start * unit, unit), size * unit)]

    def move(which, kind, owner, start, size, device):
        block = piece(which, owner, start, size)
        copy = remote(block, block, m_send.at[which, kind], m_recv.at[which, kind], device)
        copy.start()
        moves.append(copy)
        return copy

    own_shard, by_y, by_x, by_z, pass_y, pass_x, pass_z = {}, {}, {}, {}, {}, {}, {}
    for w in range(2):
        by_y[w] = move(w, 0, col, fourth, 1, over_y)
    for w in range(2):
        own_shard[w] = move(w, 1, col, 0, 4, on_chip)

    def spread_x(w):
        def run():
            by_y[w].wait_recv()
            by_x[w] = move(w, 2, across, fourth, 1, peer[1])
            pass_y[w] = move(w, 3, across, fourth, 1, on_chip)

        return run

    def spread_z(w):
        def run():
            by_x[w].wait_recv()
            other = fourth + 1 - 2 * (fourth % 2)
            by_z[w] = move(w, 4, across, 2 * (fourth // 2), 2, peer[2])
            pass_x[w] = move(w, 5, across, other, 1, on_chip)

        return run

    def pass_on(w):
        def run():
            by_z[w].wait_recv()
            pass_z[w] = move(w, 6, across, 2 - 2 * (fourth // 2), 2, on_chip)

        return run

    def gathered(w):
        for copy in (own_shard[w], pass_y[w], pass_x[w], pass_z[w]):
            copy.wait_recv()

    def make_table():
        loads["scores"].wait()
        weight_first = jax.nn.sigmoid(scores[0:1] - scores[1:2])
        for k in range(0, count, 2):
            blocks = []
            for i in (k, k + 1):
                weight = jnp.where(first == peer[i][0], weight_first, 1.0 - weight_first)
                blocks.append(jnp.where(place == rank_at(i), weight, 0.0))
            table = jnp.concatenate(blocks, axis=0).T
            top = table.astype(BF16)
            columns = slice(k * capacity, (k + 2) * capacity)
            high[:, columns] = top
            low[:, columns] = (table - top.astype(F32)).astype(BF16)

    def arrive(start, stop):
        def run():
            for k in range(max(start, 1), stop):
                sides[k].wait_recv()
                corners[k].wait_recv()

        return run

    weights_ready = set()

    def ready(name):
        if name not in weights_ready:
            weights_ready.add(name)
            loads[name].wait()

    to_side, to_own, to_y, to_ep = {}, {}, {}, {}

    def expert_steps(start, stop):
        size = (stop - start) * capacity

        def up(j):
            def run():
                ready(f"gate{j}")
                ready(f"up{j}")
                both = jnp.dot(
                    landed[start:stop].reshape(size, width), w_in[j], preferred_element_type=F32
                )
                gate = both[:, :128]
                hidden[:size, 128 * j : 128 * j + 128] = (
                    gate / (1.0 + jnp.exp(-gate)) * both[:, 128:]
                ).astype(BF16)

            return run

        def down(i, which):
            def run():
                ready("down")
                for h in range(0, quarter, 256):
                    columns = pl.ds(pl.multiple_of(which * quarter + h, 256), 256)
                    part[start:stop, i, :, h : h + 256] = (
                        jnp.dot(hidden[:size], w_down[:, columns], preferred_element_type=F32)
                        .astype(BF16)
                        .reshape(stop - start, capacity, 256)
                    )
                for k in range(start, stop):
                    if i == 1:
                        to_side[k] = remote(
                            part.at[k, 0], side_y.at[k], c_send.at[0, k], c_recv.at[0, k], on_chip
                        )
                        to_side[k].start()
                    if i == 2:
                        to_own[k] = remote(
                            part.at[k, 1], side_own.at[k], c_send.at[1, k], c_recv.at[1, k], on_chip
                        )
                        to_own[k].start()

            return run

        return [up(j) for j in range(tiles)] + [
            down(i, q) for i, q in enumerate((corner, partner, across, col))
        ]

    def add_y(ks):
        def run():
            for k in ks:
                to_side[k].wait_recv()
                sums_y[k] = (part[k, 2].astype(F32) + side_y[k].astype(F32)).astype(BF16)
            for k in ks:
                to_y[k] = remote(
                    sums_y.at[k], from_y.at[k], c_send.at[2, k], c_recv.at[2, k], over_y
                )
                to_y[k].start()

        return run

    def add_all(ks):
        def run():
            for k in ks:
                to_own[k].wait_recv()
                to_y[k].wait_recv()
                total = (
                    part[k, 3].astype(F32) + side_own[k].astype(F32) + from_y[k].astype(F32)
                ).astype(BF16)
                if k:
                    sums[k] = total
                else:
                    slots[0] = total
            for k in ks:
                if k:
                    to_ep[k] = remote(
                        sums.at[k], slots.at[k], c_send.at[3, k], c_recv.at[3, k], peer[k]
                    )
                    to_ep[k].start()

        return run

    halo = {}

    def mix_norm():
        loads["x1"].wait()
        loads["gain1"].wait()
        normalize(x1, gain1, n1)

    def mix_in():
        gathered(0)
        for n in range(0, m1.shape[1], 256):
            padded[16 : 16 + rows, n : n + 256] = jnp.dot(
                n1[...], m1[:, n : n + 256], preferred_element_type=F32
            ).astype(BF16)

    def mix_edges():
        halo[0] = remote(
            padded.at[pl.ds(rows, 16)], padded.at[pl.ds(0, 16)], h_send.at[0], h_recv.at[0],
            after_device,
        )
        halo[0].start()
        halo[1] = remote(
            padded.at[pl.ds(16, 16)], padded.at[pl.ds(16 + rows, 16)], h_send.at[1], h_recv.at[1],
            before_device,
        )
        halo[1].start()

    def mix_centre():
        halo[0].wait_recv()
        halo[1].wait_recv()
        loads["maps"].wait()
        loads["scale"].wait()
        seq_length = rows * devices // SEQS
        opening = (index * rows) % seq_length
        keep_low = (opening > 0).astype(F32)
        keep_high = (opening + rows < seq_length).astype(F32)
        floats[16 : 16 + rows] = padded[16 : 16 + rows].astype(F32)
        low_rows, high_rows = padded[:16].astype(F32), padded[16 + rows :].astype(F32)
        floats[:16] = jnp.where(keep_low > 0, low_rows, 0.0)
        floats[16 + rows :] = jnp.where(keep_high > 0, high_rows, 0.0)
        position = opening + lax.broadcasted_iota(jnp.int32, (rows, 128), 0)
        lane = lax.broadcasted_iota(jnp.int32, (rows, 128), 1)
        line = lax.broadcasted_iota(jnp.int32, (128, 128), 0)
        across_lane = lax.broadcasted_iota(jnp.int32, (128, 128), 1)
        copies = (
            lax.broadcasted_iota(jnp.int32, (GROUP, 128), 0)
            == lax.broadcasted_iota(jnp.int32, (GROUP, 128), 1) % GROUP
        ).astype(F32).astype(BF16)
        for b in range(padded.shape[1] // 128):
            columns = slice(128 * b, 128 * b + 128)

            def window(span):
                total = floats[16 - span : 16 - span + rows, columns]
                for step in range(-span + 1, span):
                    total = total + floats[16 + step : 16 + step + rows, columns]
                held = jnp.minimum(position + span, seq_length) - jnp.maximum(position - span, 0)
                return total / held.astype(F32)

            small = 1 if b % 2 == 0 else 4
            mean = jnp.where(lane < GROUP, window(small), window(2 * small))
            centred = (mean - floats[16 : 16 + rows, columns]).astype(BF16)
            spread = jnp.dot(maps[columns], copies, preferred_element_type=F32)
            block = jnp.where(line // GROUP == across_lane // GROUP, spread, 0.0).astype(BF16)
            grouped[:, columns] = (
                jnp.dot(centred, block, preferred_element_type=F32) * scale[:, columns]
            ).astype(BF16)

    def mix_out():
        gathered(1)
        for n in range(0, width, 256):
            mixed[:, n : n + 256] = jnp.dot(
                grouped[...], m2[:, n : n + 256], preferred_element_type=F32
            ).astype(BF16)

    stores = []

    def keep(source, target):
        copy = pltpu.make_async_copy(source, target, store.at[len(stores)])
        copy.start()
        stores.append(copy)

    run_schedule(
        forward, turn, spread_x, spread_z, pass_on, make_table, arrive, expert_steps, add_y,
        add_all, mix_norm, mix_in, mix_edges, mix_centre, mix_out,
        lambda: keep(mixed, mixed_hbm),
    )

    for k in EP_ORDER:
        to_ep[k].wait_recv()
    half = rows // 2
    out_y, out_side, out_corner = {}, {}, {}
    for h in range(2):
        held = slice(h * half, h * half + half)
        returned = slots[...].reshape(count * capacity, quarter)
        pieces[col, held] = (
            jnp.dot(high[held], returned, preferred_element_type=F32)
            + jnp.dot(low[held], returned, preferred_element_type=F32)
        ).astype(BF16)
    for h in range(2):
        block = pieces.at[col, pl.ds(h * half, half)]
        out_y[h] = remote(block, block, f_send.at[0, h], f_recv.at[0, h], over_y)
        out_y[h].start()
    for h in range(2):
        block = pieces.at[col, pl.ds(h * half, half)]
        out_side[h] = remote(block, block, f_send.at[1, h], f_recv.at[1, h], on_chip)
        out_side[h].start()

    def quarter_of(which):
        return result_hbm.at[:, pl.ds(pl.multiple_of(which * quarter, quarter), quarter)]

    keep(pieces.at[col], quarter_of(col))
    for h in range(2):
        out_y[h].wait_recv()
        block = pieces.at[across, pl.ds(h * half, half)]
        out_corner[h] = remote(block, block, f_send.at[2, h], f_recv.at[2, h], on_chip)
        out_corner[h].start()
    keep(pieces.at[across], quarter_of(across))
    for h in range(2):
        out_side[h].wait_recv()
    keep(pieces.at[partner], quarter_of(partner))
    for h in range(2):
        out_corner[h].wait_recv()
    keep(pieces.at[corner], quarter_of(corner))

    for k in range(count):
        to_side[k].wait_send()
        to_own[k].wait_send()
        to_y[k].wait_send()
        if k:
            firsts[k].wait_send()
            ys[k].wait_send()
            sides[k].wait_send()
            corners[k].wait_send()
            to_ep[k].wait_send()
    for copy in moves:
        copy.wait_send()
    for i in range(2):
        halo[i].wait_send()
        out_y[i].wait_send()
        out_side[i].wait_send()
        out_corner[i].wait_send()
    for copy in stores:
        copy.wait()


FIRST_ORDER = (4, 5, 1, 2, 3, 6, 7)
EP_ORDER = (1, 2, 3, 4, 5, 6, 7)


def run_schedule(
    forward, turn, spread_x, spread_z, pass_on, make_table, arrive, expert_steps, add_y,
    add_all, mix_norm, mix_in, mix_edges, mix_centre, mix_out, keep_mixed,
):
    make_table()
    mix_norm()
    for step in (forward(1), forward(4), forward(2), turn(1), forward(3), spread_x(0)):
        step()
    arrive(0, 2)()
    weave(expert_steps(0, 2), [turn(2), forward(5), turn(3), spread_x(1)])
    arrive(2, 4)()
    weave(expert_steps(2, 4), [turn(4), add_y((1, 0)), forward(6), turn(5)])
    arrive(4, 6)()
    weave(
        expert_steps(4, 6),
        [add_y((2, 3)), forward(7), turn(6), add_all((1, 0)), spread_z(0), spread_z(1), turn(7)],
    )
    arrive(6, 8)()
    weave(expert_steps(6, 8), [add_y((4, 5)), add_all((2, 3))])
    add_all((4, 5))()
    add_y((6, 7))()
    pass_on(0)()
    add_all((6, 7))()
    mix_in()
    mix_edges()
    pass_on(1)()
    mix_centre()
    mix_out()
    keep_mixed()


def fused(
    first_batch, mixer_gain, mixer_in, group_maps, pool_scale, mixer_out,
    second_batch, expert_gain, expert_choice, route_scores, expert_gate, expert_up, expert_down,
):
    rows, width = second_batch.shape
    count = lax.axis_size("ep")
    channels = pool_scale.shape[0]
    ff = expert_gate.shape[2]
    share = rows // count
    capacity = 4 * share
    quarter = width // 4
    tiles = ff // 128
    chunk = pltpu.VMEM((count, capacity, quarter), BF16)
    dma = pltpu.SemaphoreType.DMA
    anywhere = pl.BlockSpec(memory_space=pl.ANY)
    operands = (
        first_batch, mixer_gain.reshape(1, width), mixer_in,
        group_maps.reshape(channels, GROUP), pool_scale.reshape(1, channels), mixer_out,
        second_batch, expert_gain.reshape(1, width), expert_choice.T, route_scores.T,
        expert_gate, expert_up, expert_down,
    )
    return pl.pallas_call(
        layer_kernel,
        out_shape=(
            jax.ShapeDtypeStruct(first_batch.shape, BF16),
            jax.ShapeDtypeStruct(second_batch.shape, BF16),
        ),
        in_specs=[anywhere] * len(operands),
        out_specs=(anywhere, anywhere),
        scratch_shapes=[
            pltpu.VMEM((rows, width), BF16),
            pltpu.VMEM((rows, width), BF16),
            pltpu.VMEM((rows, width), BF16),
            pltpu.VMEM((rows, width), BF16),
            pltpu.VMEM((1, width), F32),
            pltpu.VMEM((1, width), F32),
            pltpu.VMEM((1, channels), F32),
            pltpu.VMEM((2, rows), jnp.int32),
            pltpu.VMEM((2, rows), F32),
            pltpu.VMEM((channels, GROUP), BF16),
            pltpu.VMEM((tiles, width, 256), BF16),
            pltpu.VMEM((ff, width), BF16),
            pltpu.VMEM((width, channels), BF16),
            pltpu.VMEM((channels, width), BF16),
            pltpu.VMEM((16, rows), F32),
            pltpu.VMEM(((count - 1) * share + capacity, rows), BF16),
            pltpu.VMEM((count - 1, share, width), BF16),
            pltpu.VMEM((count, 4, share, width), BF16),
            pltpu.VMEM((4 * capacity, ff), BF16),
            pltpu.VMEM((count, 4, capacity, quarter), BF16),
        ]
        + [chunk] * 6
        + [
            pltpu.VMEM((rows, count * capacity), BF16),
            pltpu.VMEM((rows, count * capacity), BF16),
            pltpu.VMEM((4, rows, quarter), BF16),
            pltpu.VMEM((rows + 32, channels), BF16),
            pltpu.VMEM((rows + 32, channels), F32),
            pltpu.VMEM((rows, channels), BF16),
            pltpu.VMEM((rows, width), BF16),
            dma((2 * tiles + 11,)),
            dma((4, count)),
            dma((4, count)),
            dma((4, count)),
            dma((4, count)),
            dma((2, 7)),
            dma((2, 7)),
            dma((2,)),
            dma((2,)),
            dma((3, 2)),
            dma((3, 2)),
            dma((5,)),
        ],
        compiler_params=pltpu.CompilerParams(
            collective_id=0, has_side_effects=True, vmem_limit_bytes=VMEM_LIMIT
        ),
        cost_estimate=pl.CostEstimate(flops=7 * 10**9, bytes_accessed=2**24, transcendentals=0),
        name="layer",
    )(*operands)


def per_device(*operands):
    if lax.axis_size("tp") == 4 and lax.axis_size("ep") == 8:
        return fused(*operands)
    return mixer_half(*operands[:6]), expert_half(*operands[6:])


def solution(mesh):
    placed = (
        P(("ep", "tp"), None),
        P(),
        P(None, "tp"),
        P(),
        P(),
        P("tp", None),
        P("ep", None),
        P(),
        P("ep", None),
        P("ep", None),
        P("ep", None, "tp"),
        P("ep", None, "tp"),
        P("ep", "tp", None),
    )
    return jax.shard_map(
        per_device,
        mesh=mesh,
        in_specs=placed,
        out_specs=(P(("ep", "tp"), None), P("ep", None)),
        check_vma=False,
    )
```

```python
import jax
import jax.numpy as jnp
from jax import lax
from jax.experimental import pallas as pl
from jax.experimental.pallas import tpu as pltpu
from jax.sharding import PartitionSpec as P

GROUP = 64
SEQS = 1


epsilon = 1e-06


def extended(block, sides, width):
    for axis, dim in sides:
        count = lax.axis_size(axis)
        forward = [(i, i + 1) for i in range(count - 1)]
        backward = [(target, source) for source, target in forward]
        low = lax.ppermute(
            lax.slice_in_dim(block, block.shape[dim] - width, None, axis=dim), axis, forward
        )
        high = lax.ppermute(lax.slice_in_dim(block, 0, width, axis=dim), axis, backward)
        block = jnp.concatenate([low, block, high], axis=dim)
    return block


def rms_scale(values, gain):
    floats = values.astype(jnp.float32)
    factor = lax.rsqrt(jnp.mean(floats * floats, axis=-1, keepdims=True) + epsilon)
    return (floats * factor * gain).astype(jnp.bfloat16)


def mixer_half(first_batch, mixer_gain, mixer_in, group_maps, pool_scale, mixer_out):
    count_rows = first_batch.shape[0]
    normed = rms_scale(first_batch, mixer_gain)
    pooled_in = jnp.dot(
        normed,
        lax.all_gather(mixer_in, "tp", axis=1, tiled=True),
        preferred_element_type=jnp.float32,
    ).astype(jnp.bfloat16)
    channels = pooled_in.shape[1]
    padded = extended(pooled_in, ((("ep", "tp"), 0),), 8).astype(jnp.float32)
    devices = lax.axis_size("ep") * lax.axis_size("tp")
    seq_length = count_rows * devices // SEQS
    first_row = (lax.axis_index("ep") * lax.axis_size("tp") + lax.axis_index("tp")) * count_rows
    places = first_row + jnp.arange(count_rows, dtype=jnp.int32)
    own_seq = places // seq_length
    group_of = jnp.arange(channels, dtype=jnp.int32) // GROUP
    half_span = jnp.left_shift(jnp.ones_like(group_of), group_of % 4)
    window_sum = jnp.zeros((count_rows, channels), jnp.float32)
    window_count = jnp.zeros((count_rows, channels), jnp.float32)
    for offset in range(-8, 8):
        inside = (
            ((places + offset) // seq_length == own_seq)[:, None]
            & (offset >= -half_span)[None, :]
            & (offset < half_span)[None, :]
        )
        window_sum = window_sum + jnp.where(
            inside, padded[8 + offset : 8 + offset + count_rows], 0.0
        )
        window_count = window_count + inside.astype(jnp.float32)
    centred = (window_sum / window_count - padded[8 : 8 + count_rows]).astype(jnp.bfloat16)
    group_count = group_maps.shape[0]
    identity = jnp.eye(group_count, dtype=jnp.bfloat16)
    block_map = jnp.einsum("gcd,gh->gchd", group_maps, identity).reshape(channels, channels)
    grouped = (jnp.dot(centred, block_map, preferred_element_type=jnp.float32) * pool_scale).astype(
        jnp.bfloat16
    )
    mixed_out = jnp.dot(
        grouped,
        lax.all_gather(mixer_out, "tp", axis=0, tiled=True),
        preferred_element_type=jnp.float32,
    )
    return mixed_out.astype(jnp.bfloat16)


def expert_half(
    second_batch, expert_gain, expert_choice, route_scores, expert_gate, expert_up, expert_down
):
    row_count = second_batch.shape[0]
    model_width = second_batch.shape[1]
    experts = lax.axis_size("ep")
    tp_count = lax.axis_size("tp")
    capacity = 4 * row_count // experts
    share = capacity // tp_count
    normed = rms_scale(second_batch, expert_gain)
    chosen = expert_choice.reshape(-1)
    one_hot = (chosen[:, None] == jnp.arange(experts, dtype=jnp.int32)[None, :]).astype(jnp.int32)
    ranking = jnp.sum(jnp.cumsum(one_hot, axis=0) * one_hot, axis=1) - 1
    slot_place = ranking * experts + chosen
    source_row = jnp.arange(chosen.shape[0], dtype=jnp.int32) // expert_choice.shape[1]
    slot_table = jnp.zeros((capacity * experts,), jnp.int32).at[slot_place].set(source_row + 1)
    outgoing = jnp.where(
        (slot_table > 0)[:, None],
        normed[jnp.maximum(slot_table - 1, 0)],
        jnp.zeros((), jnp.bfloat16),
    )
    outgoing = outgoing.reshape(capacity, experts, model_width)
    portion = lax.dynamic_slice_in_dim(outgoing, lax.axis_index("tp") * share, share, 0)
    arrived_part = lax.all_to_all(portion, "ep", split_axis=1, concat_axis=1, tiled=True)
    arrived = lax.all_gather(arrived_part, "tp", axis=0, tiled=True)
    incoming = arrived.reshape(capacity * experts, model_width)
    gate_weight = expert_gate[0]
    up_weight = expert_up[0]
    down_weight = expert_down[0]
    gate_part = jnp.dot(incoming, gate_weight, preferred_element_type=jnp.float32)
    up_part = jnp.dot(incoming, up_weight, preferred_element_type=jnp.float32)
    hidden = (jax.nn.silu(gate_part) * up_part).astype(jnp.bfloat16)
    summed = lax.psum_scatter(
        jnp.dot(hidden, down_weight, preferred_element_type=jnp.float32).astype(jnp.bfloat16),
        "tp",
        scatter_dimension=0,
        tiled=True,
    )
    finished = summed.reshape(share, experts, model_width)
    returned = lax.all_to_all(finished, "ep", split_axis=1, concat_axis=1, tiled=True)
    every_slot = lax.all_gather(returned, "tp", axis=0, tiled=True).reshape(
        capacity * experts, model_width
    )
    picked = every_slot[slot_place].reshape(row_count, -1, model_width)
    weight_first = jax.nn.sigmoid(route_scores[:, 0] - route_scores[:, 1])[:, None]
    blended = weight_first * picked[:, 0].astype(jnp.float32) + (1.0 - weight_first) * picked[
        :, 1
    ].astype(jnp.float32)
    return blended.astype(jnp.bfloat16)


MESH = pl.DeviceIdType.MESH
VMEM_LIMIT = 60 * 1024 * 1024
F32 = jnp.float32
BF16 = jnp.bfloat16


def flip(row, relation):
    place = row
    for bit in (1, 2, 4):
        if relation & bit:
            place = place + bit * (1 - 2 * ((row // bit) % 2))
    return place


def normalize(source, gain, target):
    for i in range(0, source.shape[0], 16):
        floats = source[i : i + 16].astype(F32)
        factor = lax.rsqrt(jnp.mean(floats * floats, axis=-1, keepdims=True) + epsilon)
        target[i : i + 16] = (floats * factor * gain[...]).astype(BF16)


def layer_kernel(
    first_hbm, mixer_gain_hbm, mixer_in_hbm, maps_hbm, scale_hbm, mixer_out_hbm,
    second_hbm, expert_gain_hbm, choice_hbm, scores_hbm, gate_hbm, up_hbm, down_hbm,
    mixed, result,
    x1, x2, n1, n2, gain1, gain2, scale, choice, scores, maps,
    w_in, w_down, m1, m2,
    rank_of, pick, portion, landed, hidden, part,
    side_y, side_own, sums_y, from_y, sums, slots, high, low, pieces,
    padded, floats, grouped,
    load, d_send, d_recv, c_send, c_recv, m_send, m_recv, h_send, h_recv, f_send, f_recv,
):
    row, col = lax.axis_index("ep"), lax.axis_index("tp")
    count = landed.shape[0]
    share = landed.shape[2]
    capacity = 4 * share
    rows, width = x2.shape
    quarter = width // 4
    tiles = w_in.shape[0]
    shard = m1.shape[1] // 4
    partner = col + 1 - 2 * (col % 2)
    across = (col + 2) % 4
    corner = (partner + 2) % 4
    devices = 4 * count
    index = row * 4 + col
    after, before = (index + 1) % devices, (index + devices - 1) % devices
    after_device, before_device = (after // 4, after % 4), (before // 4, before % 4)
    peer = [(flip(row, k), col) for k in range(count)]
    on_chip, over_y = (row, partner), (row, across)

    at = {k: i for i, k in enumerate(ORDER)}

    def remote(source, target, send, recv, device):
        return pltpu.make_async_remote_copy(
            src_ref=source, dst_ref=target, send_sem=send, recv_sem=recv,
            device_id=device, device_id_type=MESH,
        )

    def shard_of(which):
        return pl.ds(pl.multiple_of(which * shard, shard), shard)

    loads = {}

    def fetch(name, source, target):
        loads[name] = pltpu.make_async_copy(source, target, load.at[len(loads)])
        loads[name].start()

    fetch("x2", second_hbm, x2)
    fetch("gain2", expert_gain_hbm, gain2)
    fetch("choice", choice_hbm, choice)
    fetch("scores", scores_hbm, scores)
    fetch("m1", mixer_in_hbm, m1.at[:, shard_of(col)])
    fetch("m2", mixer_out_hbm, m2.at[shard_of(col)])
    fetch("x1", first_hbm, x1)
    fetch("gain1", mixer_gain_hbm, gain1)
    fetch("maps", maps_hbm, maps)
    fetch("scale", scale_hbm, scale)
    for j in range(tiles):
        fetch(f"gate{j}", gate_hbm.at[0, :, pl.ds(128 * j, 128)], w_in.at[j, :, pl.ds(0, 128)])
        fetch(f"up{j}", up_hbm.at[0, :, pl.ds(128 * j, 128)], w_in.at[j, :, pl.ds(128, 128)])
    fetch("down", down_hbm.at[0], w_down)

    barrier = pltpu.get_barrier_semaphore()
    peers = peer[1:] + [on_chip, over_y, after_device, before_device]
    for device in peers:
        pl.semaphore_signal(barrier, inc=1, device_id=device, device_id_type=MESH)

    loads["choice"].wait()
    experts = lax.broadcasted_iota(jnp.int32, (16, rows), 0)
    first, second = choice[0:1], choice[1:2]
    named = (first == experts) | (second == experts)
    earlier = lax.broadcasted_iota(jnp.int32, (rows, rows), 0) < lax.broadcasted_iota(
        jnp.int32, (rows, rows), 1
    )
    rank = jnp.dot(
        named.astype(F32).astype(BF16), earlier.astype(F32).astype(BF16), preferred_element_type=F32
    )
    rank_of[...] = jnp.where(named, rank, -1.0)

    def rank_at(k):
        return rank_of[pl.ds(peer[k][0], 1), :]

    place = lax.broadcasted_iota(jnp.int32, (capacity, rows), 0).astype(F32)
    core = col % 2
    offset = (col * share).astype(F32)
    for k in range(2, count):
        chosen = place[:share] + offset == rank_at(k)
        pick[(k - 2) * share : (k - 1) * share] = chosen.astype(F32).astype(BF16)
    far = (count - 2) * share
    pair = (core * 2 * share).astype(F32)
    chosen = place[: 2 * share] + pair == rank_at(1)
    pick[far : far + 2 * share] = chosen.astype(F32).astype(BF16)
    own = far + 2 * share
    pick[own:] = (place == rank_at(0)).astype(F32).astype(BF16)

    loads["x2"].wait()
    loads["gain2"].wait()
    normalize(x2, gain2, n2)
    for n in range(0, width, 256):
        taken = jnp.dot(pick[...], n2[:, n : n + 256], preferred_element_type=F32).astype(BF16)
        portion[:, :, n : n + 256] = taken[:own].reshape(count, share, 256)
        landed[at[0], :, :, n : n + 256] = taken[own:].reshape(4, share, 256)

    loads["m1"].wait()
    loads["m2"].wait()
    pl.semaphore_wait(barrier, len(peers))

    firsts, ys, sides, corners = {}, {}, {}, {}
    halves = landed.at[at[1], pl.ds(2 * core, 2)]
    for k in FIRST_ORDER:
        if k == 1:
            source, target = portion.at[pl.ds(count - 2, 2)], halves
        else:
            source, target = portion.at[k - 2], landed.at[at[k], col]
        firsts[k] = remote(source, target, d_send.at[0, k], d_recv.at[0, k], peer[k])
        firsts[k].start()

    def forward(k):
        firsts[k].wait_recv()
        if k == 1:
            sides[k] = remote(halves, halves, d_send.at[2, k], d_recv.at[2, k], on_chip)
            sides[k].start()
            return
        block = landed.at[at[k], col]
        ys[k] = remote(block, block, d_send.at[1, k], d_recv.at[1, k], over_y)
        ys[k].start()
        sides[k] = remote(block, block, d_send.at[2, k], d_recv.at[2, k], on_chip)
        sides[k].start()

    def turn(k):
        ys[k].wait_recv()
        block = landed.at[at[k], across]
        corners[k] = remote(block, block, d_send.at[3, k], d_recv.at[3, k], on_chip)
        corners[k].start()

    fourth = row % 4
    moves = []

    def piece(which, owner, start, size):
        if which == 0:
            unit = m1.shape[0] // 4
            return m1.at[pl.ds(pl.multiple_of(start * unit, unit), size * unit), shard_of(owner)]
        unit = shard // 4
        return m2.at[pl.ds(pl.multiple_of(owner * shard + start * unit, unit), size * unit)]

    def move(which, kind, owner, start, size, device):
        block = piece(which, owner, start, size)
        copy = remote(block, block, m_send.at[which, kind], m_recv.at[which, kind], device)
        copy.start()
        moves.append(copy)
        return copy

    own_shard, by_y, by_x, by_z, pass_y, pass_x, pass_z = {}, {}, {}, {}, {}, {}, {}
    for w in range(2):
        by_y[w] = move(w, 0, col, fourth, 1, over_y)
    for w in range(2):
        own_shard[w] = move(w, 1, col, 0, 4, on_chip)

    def spread_x(w):
        by_y[w].wait_recv()
        by_x[w] = move(w, 2, across, fourth, 1, peer[1])
        pass_y[w] = move(w, 3, across, fourth, 1, on_chip)

    def spread_z(w):
        by_x[w].wait_recv()
        other = fourth + 1 - 2 * (fourth % 2)
        by_z[w] = move(w, 4, across, 2 * (fourth // 2), 2, peer[2])
        pass_x[w] = move(w, 5, across, other, 1, on_chip)

    def pass_on(w):
        by_z[w].wait_recv()
        pass_z[w] = move(w, 6, across, 2 - 2 * (fourth // 2), 2, on_chip)

    def gathered(w):
        for copy in (own_shard[w], pass_y[w], pass_x[w], pass_z[w]):
            copy.wait_recv()

    def make_table():
        loads["scores"].wait()
        weight_first = jax.nn.sigmoid(scores[0:1] - scores[1:2])
        for k in range(0, count, 2):
            blocks = []
            for i in ORDER[k : k + 2]:
                weight = jnp.where(first == peer[i][0], weight_first, 1.0 - weight_first)
                blocks.append(jnp.where(place == rank_at(i), weight, 0.0))
            table = jnp.concatenate(blocks, axis=0).T
            top = table.astype(BF16)
            columns = slice(k * capacity, (k + 2) * capacity)
            high[:, columns] = top
            low[:, columns] = (table - top.astype(F32)).astype(BF16)

    def arrive(start, stop):
        for k in ORDER[start:stop]:
            if k:
                sides[k].wait_recv()
            if k > 1:
                corners[k].wait_recv()

    weights_ready = set()

    def ready(name):
        if name not in weights_ready:
            weights_ready.add(name)
            loads[name].wait()

    to_side, to_own, to_y, to_ep = {}, {}, {}, {}

    def raise_up(start, stop):
        size = (stop - start) * capacity
        for j in range(tiles):
            ready(f"gate{j}")
            ready(f"up{j}")
        for j in range(tiles):
            both = jnp.dot(
                landed[start:stop].reshape(size, width), w_in[j], preferred_element_type=F32
            )
            gate = both[:, :128]
            hidden[:size, 128 * j : 128 * j + 128] = (
                gate / (1.0 + jnp.exp(-gate)) * both[:, 128:]
            ).astype(BF16)

    def lower(start, stop, chosen):
        ready("down")
        size = (stop - start) * capacity
        for i in chosen:
            which = (corner, partner, across, col)[i]
            for h in range(0, quarter, 256):
                columns = pl.ds(pl.multiple_of(which * quarter + h, 256), 256)
                part[start:stop, i, :, h : h + 256] = (
                    jnp.dot(hidden[:size], w_down[:, columns], preferred_element_type=F32)
                    .astype(BF16)
                    .reshape(stop - start, capacity, 256)
                )

    def share_part(start, stop):
        for i, k in enumerate(ORDER[start:stop], start):
            to_side[k] = remote(
                part.at[i, 0], side_y.at[i], c_send.at[0, k], c_recv.at[0, k], on_chip
            )
            to_side[k].start()
        for i, k in enumerate(ORDER[start:stop], start):
            to_own[k] = remote(
                part.at[i, 1], side_own.at[i], c_send.at[1, k], c_recv.at[1, k], on_chip
            )
            to_own[k].start()

    def expert(start, stop, between=()):
        raise_up(start, stop)
        for step in between:
            step()
        lower(start, stop, (0, 1))
        share_part(start, stop)
        lower(start, stop, (2, 3))

    def add_y(*ks):
        for k in ks:
            i = at[k]
            to_side[k].wait_recv()
            sums_y[i] = (part[i, 2].astype(F32) + side_y[i].astype(F32)).astype(BF16)
            to_y[k] = remote(sums_y.at[i], from_y.at[i], c_send.at[2, k], c_recv.at[2, k], over_y)
            to_y[k].start()

    def add_all(*ks):
        for k in ks:
            i = at[k]
            to_own[k].wait_recv()
            to_y[k].wait_recv()
            total = (
                part[i, 3].astype(F32) + side_own[i].astype(F32) + from_y[i].astype(F32)
            ).astype(BF16)
            if k == 0:
                slots[i] = total
                continue
            sums[i] = total
            to_ep[k] = remote(sums.at[i], slots.at[i], c_send.at[3, k], c_recv.at[3, k], peer[k])
            to_ep[k].start()

    halo = {}

    def mix_norm():
        loads["x1"].wait()
        loads["gain1"].wait()
        normalize(x1, gain1, n1)

    def mix_in():
        gathered(0)
        for n in range(0, m1.shape[1], 256):
            padded[16 : 16 + rows, n : n + 256] = jnp.dot(
                n1[...], m1[:, n : n + 256], preferred_element_type=F32
            ).astype(BF16)

    def mix_edges():
        halo[0] = remote(
            padded.at[pl.ds(rows, 16)], padded.at[pl.ds(0, 16)], h_send.at[0], h_recv.at[0],
            after_device,
        )
        halo[0].start()
        halo[1] = remote(
            padded.at[pl.ds(16, 16)], padded.at[pl.ds(16 + rows, 16)], h_send.at[1], h_recv.at[1],
            before_device,
        )
        halo[1].start()

    def mix_centre():
        halo[0].wait_recv()
        halo[1].wait_recv()
        loads["maps"].wait()
        loads["scale"].wait()
        seq_length = rows * devices // SEQS
        opening = (index * rows) % seq_length
        keep_low = (opening > 0).astype(F32)
        keep_high = (opening + rows < seq_length).astype(F32)
        floats[16 : 16 + rows] = padded[16 : 16 + rows].astype(F32)
        low_rows, high_rows = padded[:16].astype(F32), padded[16 + rows :].astype(F32)
        floats[:16] = jnp.where(keep_low > 0, low_rows, 0.0)
        floats[16 + rows :] = jnp.where(keep_high > 0, high_rows, 0.0)
        position = opening + lax.broadcasted_iota(jnp.int32, (rows, 128), 0)
        lane = lax.broadcasted_iota(jnp.int32, (rows, 128), 1)
        line = lax.broadcasted_iota(jnp.int32, (128, 128), 0)
        across_lane = lax.broadcasted_iota(jnp.int32, (128, 128), 1)
        copies = (
            lax.broadcasted_iota(jnp.int32, (GROUP, 128), 0)
            == lax.broadcasted_iota(jnp.int32, (GROUP, 128), 1) % GROUP
        ).astype(F32).astype(BF16)
        for b in range(padded.shape[1] // 128):
            columns = slice(128 * b, 128 * b + 128)

            def window(span):
                total = floats[16 - span : 16 - span + rows, columns]
                for step in range(-span + 1, span):
                    total = total + floats[16 + step : 16 + step + rows, columns]
                held = jnp.minimum(position + span, seq_length) - jnp.maximum(position - span, 0)
                return total / held.astype(F32)

            small = 1 if b % 2 == 0 else 4
            mean = jnp.where(lane < GROUP, window(small), window(2 * small))
            centred = (mean - floats[16 : 16 + rows, columns]).astype(BF16)
            spread = jnp.dot(maps[columns], copies, preferred_element_type=F32)
            block = jnp.where(line // GROUP == across_lane // GROUP, spread, 0.0).astype(BF16)
            grouped[:, columns] = (
                jnp.dot(centred, block, preferred_element_type=F32) * scale[:, columns]
            ).astype(BF16)

    def mix_out():
        gathered(1)
        for n in range(0, width, 256):
            mixed[:, n : n + 256] = jnp.dot(
                grouped[...], m2[:, n : n + 256], preferred_element_type=F32
            ).astype(BF16)

    make_table()
    mix_norm()
    forward(2)
    forward(1)
    arrive(0, 2)
    expert(0, 2, [lambda: forward(4)])
    forward(3)
    spread_x(0)
    spread_x(1)
    turn(2)
    forward(5)
    turn(4)
    forward(6)
    add_y(1)
    arrive(2, 4)
    expert(2, 4, [lambda: turn(3), lambda: forward(7)])
    spread_z(0)
    add_y(4, 2)
    turn(5)
    add_all(1)
    arrive(4, 6)
    expert(4, 6, [lambda: turn(6)])
    add_y(5)
    turn(7)
    add_all(4)
    arrive(6, 8)
    expert(6, 8, [lambda: add_all(2)])
    add_y(7, 6, 3, 0)
    add_all(5)
    pass_on(0)
    mix_in()
    mix_edges()
    add_all(7, 6, 3)
    spread_z(1)
    add_all(0)
    mix_centre()

    for k in ORDER:
        if k:
            to_ep[k].wait_recv()
    half = rows // 2
    out_y, out_side, out_corner = {}, {}, {}
    for h in range(2):
        held = slice(h * half, h * half + half)
        returned = slots[...].reshape(count * capacity, quarter)
        pieces[col, held] = (
            jnp.dot(high[held], returned, preferred_element_type=F32)
            + jnp.dot(low[held], returned, preferred_element_type=F32)
        ).astype(BF16)
    for h in range(2):
        block = pieces.at[col, pl.ds(h * half, half)]
        out_y[h] = remote(block, block, f_send.at[0, h], f_recv.at[0, h], over_y)
        out_y[h].start()
    for h in range(2):
        block = pieces.at[col, pl.ds(h * half, half)]
        out_side[h] = remote(block, block, f_send.at[1, h], f_recv.at[1, h], on_chip)
        out_side[h].start()

    def place_piece(which):
        columns = pl.ds(pl.multiple_of(which * quarter, quarter), quarter)
        result[:, columns] = pieces[which]

    place_piece(col)
    for h in range(2):
        out_y[h].wait_recv()
        block = pieces.at[across, pl.ds(h * half, half)]
        out_corner[h] = remote(block, block, f_send.at[2, h], f_recv.at[2, h], on_chip)
        out_corner[h].start()
    place_piece(across)
    pass_on(1)
    mix_out()
    for h in range(2):
        out_side[h].wait_recv()
    place_piece(partner)
    for h in range(2):
        out_corner[h].wait_recv()
    place_piece(corner)

    for k in range(count):
        to_side[k].wait_send()
        to_own[k].wait_send()
        to_y[k].wait_send()
        if k:
            firsts[k].wait_send()
            sides[k].wait_send()
            to_ep[k].wait_send()
        if k > 1:
            ys[k].wait_send()
            corners[k].wait_send()
    for copy in moves:
        copy.wait_send()
    for i in range(2):
        halo[i].wait_send()
        out_y[i].wait_send()
        out_side[i].wait_send()
        out_corner[i].wait_send()


FIRST_ORDER = (1, 4, 5, 2, 3, 6, 7)
ORDER = (1, 0, 4, 2, 5, 3, 6, 7)


def finish_kernel(mixed, result, mixed_out, result_out, held, into, out):
    step = held.shape[1] // 4
    loads, stores = [], []
    for i, source in enumerate((result, mixed)):
        for j in range(4):
            rows = pl.ds(step * j, step)
            copy = pltpu.make_async_copy(source.at[rows], held.at[i, rows], into.at[4 * i + j])
            copy.start()
            loads.append(copy)
    for i, target in enumerate((result_out, mixed_out)):
        for j in range(4):
            rows = pl.ds(step * j, step)
            loads[4 * i + j].wait()
            copy = pltpu.make_async_copy(held.at[i, rows], target.at[rows], out.at[4 * i + j])
            copy.start()
            stores.append(copy)
    for copy in stores:
        copy.wait()


def finish(mixed, result):
    anywhere = pl.BlockSpec(memory_space=pl.ANY)
    return pl.pallas_call(
        finish_kernel,
        out_shape=tuple(jax.ShapeDtypeStruct(x.shape, x.dtype) for x in (mixed, result)),
        in_specs=[anywhere] * 2,
        out_specs=(anywhere, anywhere),
        scratch_shapes=[
            pltpu.VMEM((2,) + result.shape, result.dtype),
            pltpu.SemaphoreType.DMA((8,)),
            pltpu.SemaphoreType.DMA((8,)),
        ],
        name="finish",
    )(mixed, result)


def fused(
    first_batch, mixer_gain, mixer_in, group_maps, pool_scale, mixer_out,
    second_batch, expert_gain, expert_choice, route_scores, expert_gate, expert_up, expert_down,
):
    rows, width = second_batch.shape
    count = lax.axis_size("ep")
    channels = pool_scale.shape[0]
    ff = expert_gate.shape[2]
    share = rows // count
    capacity = 4 * share
    quarter = width // 4
    tiles = ff // 128
    chunk = pltpu.VMEM((count, capacity, quarter), BF16)
    dma = pltpu.SemaphoreType.DMA
    in_hbm = pl.BlockSpec(memory_space=pltpu.HBM)
    in_vmem = pl.BlockSpec(memory_space=pltpu.VMEM)
    operands = (
        first_batch, mixer_gain.reshape(1, width), mixer_in,
        group_maps.reshape(channels, GROUP), pool_scale.reshape(1, channels), mixer_out,
        second_batch, expert_gain.reshape(1, width), expert_choice.T, route_scores.T,
        expert_gate, expert_up, expert_down,
    )
    return finish(*pl.pallas_call(
        layer_kernel,
        out_shape=(
            jax.ShapeDtypeStruct(first_batch.shape, BF16),
            jax.ShapeDtypeStruct(second_batch.shape, BF16),
        ),
        in_specs=[in_hbm] * len(operands),
        out_specs=(in_vmem, in_vmem),
        scratch_shapes=[
            pltpu.VMEM((rows, width), BF16),
            pltpu.VMEM((rows, width), BF16),
            pltpu.VMEM((rows, width), BF16),
            pltpu.VMEM((rows, width), BF16),
            pltpu.VMEM((1, width), F32),
            pltpu.VMEM((1, width), F32),
            pltpu.VMEM((1, channels), F32),
            pltpu.VMEM((2, rows), jnp.int32),
            pltpu.VMEM((2, rows), F32),
            pltpu.VMEM((channels, GROUP), BF16),
            pltpu.VMEM((tiles, width, 256), BF16),
            pltpu.VMEM((ff, width), BF16),
            pltpu.VMEM((width, channels), BF16),
            pltpu.VMEM((channels, width), BF16),
            pltpu.VMEM((16, rows), F32),
            pltpu.VMEM((count * share + capacity, rows), BF16),
            pltpu.VMEM((count, share, width), BF16),
            pltpu.VMEM((count, 4, share, width), BF16),
            pltpu.VMEM((4 * capacity, ff), BF16),
            pltpu.VMEM((count, 4, capacity, quarter), BF16),
        ]
        + [chunk] * 6
        + [
            pltpu.VMEM((rows, count * capacity), BF16),
            pltpu.VMEM((rows, count * capacity), BF16),
            pltpu.VMEM((4, rows, quarter), BF16),
            pltpu.VMEM((rows + 32, channels), BF16),
            pltpu.VMEM((rows + 32, channels), F32),
            pltpu.VMEM((rows, channels), BF16),
            dma((2 * tiles + 11,)),
            dma((4, count)),
            dma((4, count)),
            dma((4, count)),
            dma((4, count)),
            dma((2, 7)),
            dma((2, 7)),
            dma((2,)),
            dma((2,)),
            dma((3, 2)),
            dma((3, 2)),
        ],
        compiler_params=pltpu.CompilerParams(
            collective_id=0, has_side_effects=True, vmem_limit_bytes=VMEM_LIMIT
        ),
        cost_estimate=pl.CostEstimate(flops=7 * 10**9, bytes_accessed=2**24, transcendentals=0),
        name="layer",
    )(*operands))


def per_device(*operands):
    if lax.axis_size("tp") == 4 and lax.axis_size("ep") == 8:
        return fused(*operands)
    return mixer_half(*operands[:6]), expert_half(*operands[6:])


def solution(mesh):
    placed = (
        P(("ep", "tp"), None),
        P(),
        P(None, "tp"),
        P(),
        P(),
        P("tp", None),
        P("ep", None),
        P(),
        P("ep", None),
        P("ep", None),
        P("ep", None, "tp"),
        P("ep", None, "tp"),
        P("ep", "tp", None),
    )
    return jax.shard_map(
        per_device,
        mesh=mesh,
        in_specs=placed,
        out_specs=(P(("ep", "tp"), None), P("ep", None)),
        check_vma=False,
    )
```

```python
import jax
import jax.numpy as jnp
from jax import lax
from jax.experimental import pallas as pl
from jax.experimental.pallas import tpu as pltpu
from jax.sharding import PartitionSpec as P

GROUP = 64
SEQS = 1


epsilon = 1e-06


def extended(block, sides, width):
    for axis, dim in sides:
        count = lax.axis_size(axis)
        forward = [(i, i + 1) for i in range(count - 1)]
        backward = [(target, source) for source, target in forward]
        low = lax.ppermute(
            lax.slice_in_dim(block, block.shape[dim] - width, None, axis=dim), axis, forward
        )
        high = lax.ppermute(lax.slice_in_dim(block, 0, width, axis=dim), axis, backward)
        block = jnp.concatenate([low, block, high], axis=dim)
    return block


def rms_scale(values, gain):
    floats = values.astype(jnp.float32)
    factor = lax.rsqrt(jnp.mean(floats * floats, axis=-1, keepdims=True) + epsilon)
    return (floats * factor * gain).astype(jnp.bfloat16)


def mixer_half(first_batch, mixer_gain, mixer_in, group_maps, pool_scale, mixer_out):
    count_rows = first_batch.shape[0]
    normed = rms_scale(first_batch, mixer_gain)
    pooled_in = jnp.dot(
        normed,
        lax.all_gather(mixer_in, "tp", axis=1, tiled=True),
        preferred_element_type=jnp.float32,
    ).astype(jnp.bfloat16)
    channels = pooled_in.shape[1]
    padded = extended(pooled_in, ((("ep", "tp"), 0),), 8).astype(jnp.float32)
    devices = lax.axis_size("ep") * lax.axis_size("tp")
    seq_length = count_rows * devices // SEQS
    first_row = (lax.axis_index("ep") * lax.axis_size("tp") + lax.axis_index("tp")) * count_rows
    places = first_row + jnp.arange(count_rows, dtype=jnp.int32)
    own_seq = places // seq_length
    group_of = jnp.arange(channels, dtype=jnp.int32) // GROUP
    half_span = jnp.left_shift(jnp.ones_like(group_of), group_of % 4)
    window_sum = jnp.zeros((count_rows, channels), jnp.float32)
    window_count = jnp.zeros((count_rows, channels), jnp.float32)
    for offset in range(-8, 8):
        inside = (
            ((places + offset) // seq_length == own_seq)[:, None]
            & (offset >= -half_span)[None, :]
            & (offset < half_span)[None, :]
        )
        window_sum = window_sum + jnp.where(
            inside, padded[8 + offset : 8 + offset + count_rows], 0.0
        )
        window_count = window_count + inside.astype(jnp.float32)
    centred = (window_sum / window_count - padded[8 : 8 + count_rows]).astype(jnp.bfloat16)
    group_count = group_maps.shape[0]
    identity = jnp.eye(group_count, dtype=jnp.bfloat16)
    block_map = jnp.einsum("gcd,gh->gchd", group_maps, identity).reshape(channels, channels)
    grouped = (jnp.dot(centred, block_map, preferred_element_type=jnp.float32) * pool_scale).astype(
        jnp.bfloat16
    )
    mixed_out = jnp.dot(
        grouped,
        lax.all_gather(mixer_out, "tp", axis=0, tiled=True),
        preferred_element_type=jnp.float32,
    )
    return mixed_out.astype(jnp.bfloat16)


def expert_half(
    second_batch, expert_gain, expert_choice, route_scores, expert_gate, expert_up, expert_down
):
    row_count = second_batch.shape[0]
    model_width = second_batch.shape[1]
    experts = lax.axis_size("ep")
    tp_count = lax.axis_size("tp")
    capacity = 4 * row_count // experts
    share = capacity // tp_count
    normed = rms_scale(second_batch, expert_gain)
    chosen = expert_choice.reshape(-1)
    one_hot = (chosen[:, None] == jnp.arange(experts, dtype=jnp.int32)[None, :]).astype(jnp.int32)
    ranking = jnp.sum(jnp.cumsum(one_hot, axis=0) * one_hot, axis=1) - 1
    slot_place = ranking * experts + chosen
    source_row = jnp.arange(chosen.shape[0], dtype=jnp.int32) // expert_choice.shape[1]
    slot_table = jnp.zeros((capacity * experts,), jnp.int32).at[slot_place].set(source_row + 1)
    outgoing = jnp.where(
        (slot_table > 0)[:, None],
        normed[jnp.maximum(slot_table - 1, 0)],
        jnp.zeros((), jnp.bfloat16),
    )
    outgoing = outgoing.reshape(capacity, experts, model_width)
    portion = lax.dynamic_slice_in_dim(outgoing, lax.axis_index("tp") * share, share, 0)
    arrived_part = lax.all_to_all(portion, "ep", split_axis=1, concat_axis=1, tiled=True)
    arrived = lax.all_gather(arrived_part, "tp", axis=0, tiled=True)
    incoming = arrived.reshape(capacity * experts, model_width)
    gate_weight = expert_gate[0]
    up_weight = expert_up[0]
    down_weight = expert_down[0]
    gate_part = jnp.dot(incoming, gate_weight, preferred_element_type=jnp.float32)
    up_part = jnp.dot(incoming, up_weight, preferred_element_type=jnp.float32)
    hidden = (jax.nn.silu(gate_part) * up_part).astype(jnp.bfloat16)
    summed = lax.psum_scatter(
        jnp.dot(hidden, down_weight, preferred_element_type=jnp.float32).astype(jnp.bfloat16),
        "tp",
        scatter_dimension=0,
        tiled=True,
    )
    finished = summed.reshape(share, experts, model_width)
    returned = lax.all_to_all(finished, "ep", split_axis=1, concat_axis=1, tiled=True)
    every_slot = lax.all_gather(returned, "tp", axis=0, tiled=True).reshape(
        capacity * experts, model_width
    )
    picked = every_slot[slot_place].reshape(row_count, -1, model_width)
    weight_first = jax.nn.sigmoid(route_scores[:, 0] - route_scores[:, 1])[:, None]
    blended = weight_first * picked[:, 0].astype(jnp.float32) + (1.0 - weight_first) * picked[
        :, 1
    ].astype(jnp.float32)
    return blended.astype(jnp.bfloat16)


MESH = pl.DeviceIdType.MESH
VMEM_LIMIT = 60 * 1024 * 1024
F32 = jnp.float32
BF16 = jnp.bfloat16


def flip(row, relation):
    place = row
    for bit in (1, 2, 4):
        if relation & bit:
            place = place + bit * (1 - 2 * ((row // bit) % 2))
    return place


def normalize(source, gain, target):
    for i in range(0, source.shape[0], 16):
        floats = source[i : i + 16].astype(F32)
        factor = lax.rsqrt(jnp.mean(floats * floats, axis=-1, keepdims=True) + epsilon)
        target[i : i + 16] = (floats * factor * gain[...]).astype(BF16)


def layer_kernel(
    first_hbm, mixer_gain_hbm, mixer_in_hbm, maps_hbm, scale_hbm, mixer_out_hbm,
    second_hbm, expert_gain_hbm, choice_hbm, scores_hbm, gate_hbm, up_hbm, down_hbm,
    mixed_hbm, result_hbm,
    x1, x2, n1, n2, gain1, gain2, scale, choice, scores, maps,
    w_in, w_down, m1, m2,
    rank_of, pick, portion, landed, hidden, part,
    side_y, side_own, sums_y, from_y, sums, slots, high, low, pieces,
    padded, floats, grouped, mixed,
    load, d_send, first_recv, y_recv, block_recv, c_send, part_recv, sum_recv, slot_recv,
    m_send, m_recv, h_send, h_recv, f_send, f_recv, store,
):
    row, col = lax.axis_index("ep"), lax.axis_index("tp")
    count = landed.shape[0]
    share = landed.shape[2]
    capacity = 4 * share
    rows, width = x2.shape
    quarter = width // 4
    tiles = w_in.shape[0]
    shard = m1.shape[1] // 4
    partner = col + 1 - 2 * (col % 2)
    across = (col + 2) % 4
    corner = (partner + 2) % 4
    devices = 4 * count
    index = row * 4 + col
    after, before = (index + 1) % devices, (index + devices - 1) % devices
    after_device, before_device = (after // 4, after % 4), (before // 4, before % 4)
    peer = [(flip(row, k), col) for k in range(count)]
    on_chip, over_y = (row, partner), (row, across)

    at = {k: i for i, k in enumerate(ORDER)}

    def remote(source, target, send, recv, device):
        return pltpu.make_async_remote_copy(
            src_ref=source, dst_ref=target, send_sem=send, recv_sem=recv,
            device_id=device, device_id_type=MESH,
        )

    def shard_of(which):
        return pl.ds(pl.multiple_of(which * shard, shard), shard)

    loads = {}

    def fetch(name, source, target):
        loads[name] = pltpu.make_async_copy(source, target, load.at[len(loads)])
        loads[name].start()

    fetch("x2", second_hbm, x2)
    fetch("gain2", expert_gain_hbm, gain2)
    fetch("choice", choice_hbm, choice)
    fetch("scores", scores_hbm, scores)
    fetch("m1", mixer_in_hbm, m1.at[:, shard_of(col)])
    fetch("m2", mixer_out_hbm, m2.at[shard_of(col)])
    fetch("x1", first_hbm, x1)
    fetch("gain1", mixer_gain_hbm, gain1)
    fetch("maps", maps_hbm, maps)
    fetch("scale", scale_hbm, scale)
    fetch("down", down_hbm.at[0], w_down)
    sem = load.at[len(loads)]
    for j in range(tiles):
        for i, source in enumerate((gate_hbm, up_hbm)):
            target = w_in.at[j, :, pl.ds(128 * i, 128)]
            pltpu.make_async_copy(source.at[0, :, pl.ds(128 * j, 128)], target, sem).start()
    loads["w_in"] = pltpu.make_async_copy(w_in, w_in, sem)

    barrier = pltpu.get_barrier_semaphore()
    peers = peer[1:] + [on_chip, over_y, after_device, before_device]
    for device in peers:
        pl.semaphore_signal(barrier, inc=1, device_id=device, device_id_type=MESH)

    loads["choice"].wait()
    experts = lax.broadcasted_iota(jnp.int32, (16, rows), 0)
    first, second = choice[0:1], choice[1:2]
    named = (first == experts) | (second == experts)
    earlier = lax.broadcasted_iota(jnp.int32, (rows, rows), 0) < lax.broadcasted_iota(
        jnp.int32, (rows, rows), 1
    )
    rank = jnp.dot(
        named.astype(F32).astype(BF16), earlier.astype(F32).astype(BF16), preferred_element_type=F32
    )
    rank_of[...] = jnp.where(named, rank, -1.0)

    def rank_at(k):
        return rank_of[pl.ds(peer[k][0], 1), :]

    place = lax.broadcasted_iota(jnp.int32, (capacity, rows), 0).astype(F32)
    core = col % 2
    offset = (col * share).astype(F32)
    for k in range(2, count):
        chosen = place[:share] + offset == rank_at(k)
        pick[(k - 2) * share : (k - 1) * share] = chosen.astype(F32).astype(BF16)
    far = (count - 2) * share
    pair = (core * 2 * share).astype(F32)
    chosen = place[: 2 * share] + pair == rank_at(1)
    pick[far : far + 2 * share] = chosen.astype(F32).astype(BF16)
    own = far + 2 * share
    pick[own:] = (place == rank_at(0)).astype(F32).astype(BF16)

    loads["x2"].wait()
    loads["gain2"].wait()
    normalize(x2, gain2, n2)
    for n in range(0, width, 256):
        taken = jnp.dot(pick[...], n2[:, n : n + 256], preferred_element_type=F32).astype(BF16)
        portion[:, :, n : n + 256] = taken[:own].reshape(count, share, 256)
        landed[at[0], :, :, n : n + 256] = taken[own:].reshape(4, share, 256)

    loads["m1"].wait()
    loads["m2"].wait()
    pl.semaphore_wait(barrier, len(peers))

    firsts, ys, sides, corners = {}, {}, {}, {}
    halves = landed.at[at[1], pl.ds(2 * core, 2)]
    for k in FIRST_ORDER:
        if k == 1:
            source, target = portion.at[pl.ds(count - 2, 2)], halves
        else:
            source, target = portion.at[k - 2], landed.at[at[k], col]
        firsts[k] = remote(source, target, d_send.at[0], first_recv.at[k], peer[k])
        firsts[k].start()

    def forward(k):
        firsts[k].wait_recv()
        if k == 1:
            sides[k] = remote(halves, halves, d_send.at[2], block_recv.at[at[k] // 2], on_chip)
            sides[k].start()
            return
        block = landed.at[at[k], col]
        ys[k] = remote(block, block, d_send.at[1], y_recv.at[k], over_y)
        ys[k].start()
        sides[k] = remote(block, block, d_send.at[2], block_recv.at[at[k] // 2], on_chip)
        sides[k].start()

    def turn(k):
        ys[k].wait_recv()
        block = landed.at[at[k], across]
        corners[k] = remote(block, block, d_send.at[3], block_recv.at[at[k] // 2], on_chip)
        corners[k].start()

    fourth = (row % 2) * 2 + (row // 2) % 2

    def piece(which, owner, start, size):
        if which == 0:
            unit = m1.shape[0] // 4
            return m1.at[pl.ds(pl.multiple_of(start * unit, unit), size * unit), shard_of(owner)]
        unit = shard // 4
        return m2.at[pl.ds(pl.multiple_of(owner * shard + start * unit, unit), size * unit)]

    def move(which, kind, owner, start, size, device):
        block = piece(which, owner, start, size)
        copy = remote(block, block, m_send.at[which], m_recv.at[which, kind], device)
        copy.start()
        return copy

    by_y, by_z, by_x = {}, {}, {}
    for w in range(2):
        by_y[w] = move(w, 0, col, fourth, 1, over_y)
    for w in range(2):
        move(w, 3, col, 0, 4, on_chip)

    def spread_z(w):
        by_y[w].wait_recv()
        by_z[w] = move(w, 1, across, fourth, 1, peer[2])
        move(w, 3, across, fourth, 1, on_chip)

    def spread_x(w):
        by_z[w].wait_recv()
        other = fourth + 1 - 2 * (fourth % 2)
        by_x[w] = move(w, 2, across, 2 * (fourth // 2), 2, peer[1])
        move(w, 3, across, other, 1, on_chip)

    def pass_on(w):
        by_x[w].wait_recv()
        move(w, 3, across, 2 - 2 * (fourth // 2), 2, on_chip)

    def whole(which, parts):
        ref = (m1, m2)[which]
        block = ref.at[pl.ds(0, ref.shape[0] * parts // 4)]
        return remote(block, block, m_send.at[which], m_recv.at[which, 3], on_chip)

    def gathered(w):
        whole(w, 2).wait_recv()

    def make_table():
        loads["scores"].wait()
        weight_first = jax.nn.sigmoid(scores[0:1] - scores[1:2])
        for k in range(0, count, 2):
            blocks = []
            for i in ORDER[k : k + 2]:
                weight = jnp.where(first == peer[i][0], weight_first, 1.0 - weight_first)
                blocks.append(jnp.where(place == rank_at(i), weight, 0.0))
            table = jnp.concatenate(blocks, axis=0).T
            top = table.astype(BF16)
            columns = slice(k * capacity, (k + 2) * capacity)
            high[:, columns] = top
            low[:, columns] = (table - top.astype(F32)).astype(BF16)

    def arrive(chunk):
        blocks = sum(2 for k in ORDER[2 * chunk : 2 * chunk + 2] if k)
        landing = landed.at[2 * chunk, pl.ds(0, blocks)]
        remote(landing, landing, d_send.at[2], block_recv.at[chunk], on_chip).wait_recv()

    weights_ready = set()

    def ready(name):
        if name not in weights_ready:
            weights_ready.add(name)
            loads[name].wait()

    to_side, to_own, to_y, to_ep = {}, {}, {}, {}

    def raise_up(start, stop, chosen):
        size = (stop - start) * capacity
        ready("w_in")
        for j in chosen:
            both = jnp.dot(
                landed[start:stop].reshape(size, width), w_in[j], preferred_element_type=F32
            )
            gate = both[:, :128]
            hidden[:size, 128 * j : 128 * j + 128] = (
                gate / (1.0 + jnp.exp(-gate)) * both[:, 128:]
            ).astype(BF16)

    def lower(start, stop, chosen):
        ready("down")
        size = (stop - start) * capacity
        for i in chosen:
            which = (corner, partner, across, col)[i]
            for h in range(0, quarter, 256):
                columns = pl.ds(pl.multiple_of(which * quarter + h, 256), 256)
                part[start:stop, i, :, h : h + 256] = (
                    jnp.dot(hidden[:size], w_down[:, columns], preferred_element_type=F32)
                    .astype(BF16)
                    .reshape(stop - start, capacity, 256)
                )

    def share_part(start, stop):
        for i, k in enumerate(ORDER[start:stop], start):
            to_side[k] = remote(
                part.at[i, 0], side_y.at[i], c_send.at[0], part_recv.at[i // 2], on_chip
            )
            to_side[k].start()
        for i, k in enumerate(ORDER[start:stop], start):
            to_own[k] = remote(
                part.at[i, 1], side_own.at[i], c_send.at[1], part_recv.at[i // 2], on_chip
            )
            to_own[k].start()

    def expert(start, stop, within=(), between=()):
        middle = tiles // 2 if within else 0
        raise_up(start, stop, range(middle))
        for step in within:
            step()
        raise_up(start, stop, range(middle, tiles))
        for step in between:
            step()
        lower(start, stop, (0, 1))
        share_part(start, stop)
        lower(start, stop, (2, 3))

    met = set()

    def halved(chunk):
        if chunk not in met:
            met.add(chunk)
            block = side_y.at[pl.ds(0, 4)]
            remote(block, block, c_send.at[0], part_recv.at[chunk], on_chip).wait_recv()

    def add_y(*ks):
        for k in ks:
            i = at[k]
            halved(i // 2)
            sums_y[i] = (part[i, 2].astype(F32) + side_y[i].astype(F32)).astype(BF16)
            to_y[k] = remote(sums_y.at[i], from_y.at[i], c_send.at[2], sum_recv.at[k], over_y)
            to_y[k].start()

    def add_all(*ks):
        for k in ks:
            i = at[k]
            to_y[k].wait_recv()
            total = (
                part[i, 3].astype(F32) + side_own[i].astype(F32) + from_y[i].astype(F32)
            ).astype(BF16)
            if k == 0:
                slots[i] = total
                continue
            sums[i] = total
            to_ep[k] = remote(sums.at[i], slots.at[i], c_send.at[3], slot_recv.at[0], peer[k])
            to_ep[k].start()

    halo = {}

    def mix_norm():
        loads["x1"].wait()
        loads["gain1"].wait()
        normalize(x1, gain1, n1)

    def mix_in():
        gathered(0)
        for n in range(0, m1.shape[1], 256):
            padded[16 : 16 + rows, n : n + 256] = jnp.dot(
                n1[...], m1[:, n : n + 256], preferred_element_type=F32
            ).astype(BF16)

    def mix_edges():
        halo[0] = remote(
            padded.at[pl.ds(rows, 16)], padded.at[pl.ds(0, 16)], h_send.at[0], h_recv.at[0],
            after_device,
        )
        halo[0].start()
        halo[1] = remote(
            padded.at[pl.ds(16, 16)], padded.at[pl.ds(16 + rows, 16)], h_send.at[0], h_recv.at[0],
            before_device,
        )
        halo[1].start()

    def both_edges():
        edges = padded.at[pl.ds(0, 32)]
        return remote(edges, edges, h_send.at[0], h_recv.at[0], after_device)

    def mix_centre():
        both_edges().wait_recv()
        loads["maps"].wait()
        loads["scale"].wait()
        seq_length = rows * devices // SEQS
        opening = (index * rows) % seq_length
        keep_low = (opening > 0).astype(F32)
        keep_high = (opening + rows < seq_length).astype(F32)
        floats[16 : 16 + rows] = padded[16 : 16 + rows].astype(F32)
        low_rows, high_rows = padded[:16].astype(F32), padded[16 + rows :].astype(F32)
        floats[:16] = jnp.where(keep_low > 0, low_rows, 0.0)
        floats[16 + rows :] = jnp.where(keep_high > 0, high_rows, 0.0)
        position = opening + lax.broadcasted_iota(jnp.int32, (rows, 128), 0)
        lane = lax.broadcasted_iota(jnp.int32, (rows, 128), 1)
        line = lax.broadcasted_iota(jnp.int32, (128, 128), 0)
        across_lane = lax.broadcasted_iota(jnp.int32, (128, 128), 1)
        copies = (
            lax.broadcasted_iota(jnp.int32, (GROUP, 128), 0)
            == lax.broadcasted_iota(jnp.int32, (GROUP, 128), 1) % GROUP
        ).astype(F32).astype(BF16)
        for b in range(padded.shape[1] // 128):
            columns = slice(128 * b, 128 * b + 128)

            def window(span):
                total = floats[16 - span : 16 - span + rows, columns]
                for step in range(-span + 1, span):
                    total = total + floats[16 + step : 16 + step + rows, columns]
                held = jnp.minimum(position + span, seq_length) - jnp.maximum(position - span, 0)
                return total / held.astype(F32)

            small = 1 if b % 2 == 0 else 4
            mean = jnp.where(lane < GROUP, window(small), window(2 * small))
            centred = (mean - floats[16 : 16 + rows, columns]).astype(BF16)
            spread = jnp.dot(maps[columns], copies, preferred_element_type=F32)
            block = jnp.where(line // GROUP == across_lane // GROUP, spread, 0.0).astype(BF16)
            grouped[:, columns] = (
                jnp.dot(centred, block, preferred_element_type=F32) * scale[:, columns]
            ).astype(BF16)

    def mix_out():
        gathered(1)
        for n in range(0, width, 256):
            mixed[:, n : n + 256] = jnp.dot(
                grouped[...], m2[:, n : n + 256], preferred_element_type=F32
            ).astype(BF16)

    make_table()
    mix_norm()
    spread_z(0)
    forward(4)
    forward(2)
    forward(1)
    forward(3)
    spread_z(1)
    turn(4)
    forward(5)
    arrive(0)
    expert(0, 2, between=[lambda: forward(6), lambda: turn(2)])
    turn(3)
    forward(7)
    spread_x(0)
    add_y(4)
    turn(5)
    arrive(1)
    expert(2, 4, between=[lambda: turn(6)])
    spread_x(1)
    arrive(2)
    expert(4, 6, [lambda: add_y(5, 1), lambda: add_all(4)], [lambda: turn(7)])
    arrive(3)
    expert(6, 8, [lambda: add_y(6, 3)], [lambda: add_all(5)])
    add_all(1)
    add_y(7, 2, 0)
    add_all(6)
    pass_on(0)
    mix_in()
    mix_edges()
    add_all(3, 7, 2, 0)
    mix_centre()
    pass_on(1)

    back = slots.at[pl.ds(0, count - 1)]
    remote(back, back, c_send.at[3], slot_recv.at[0], on_chip).wait_recv()
    bits = rows // 4
    out_y = {}
    returned = slots[...].reshape(count * capacity, quarter)
    pieces[col] = (
        jnp.dot(high[...], returned, preferred_element_type=F32)
        + jnp.dot(low[...], returned, preferred_element_type=F32)
    ).astype(BF16)
    for h in range(4):
        block = pieces.at[col, pl.ds(h * bits, bits)]
        out_y[h] = remote(block, block, f_send.at[0], f_recv.at[h], over_y)
        out_y[h].start()
    own_piece = pieces.at[col]
    out_side = remote(own_piece, own_piece, f_send.at[0], f_recv.at[4], on_chip)
    out_side.start()

    def place_piece(which):
        columns = pl.ds(pl.multiple_of(which * quarter, quarter), quarter)
        pltpu.make_async_copy(pieces.at[which], result_hbm.at[:, columns], store.at[0]).start()

    place_piece(col)
    for h in range(4):
        out_y[h].wait_recv()
        block = pieces.at[across, pl.ds(h * bits, bits)]
        remote(block, block, f_send.at[0], f_recv.at[5], on_chip).start()
    place_piece(across)
    out_side.wait_recv()
    place_piece(partner)
    mix_out()
    mixed_store = pltpu.make_async_copy(mixed, mixed_hbm, store.at[1])
    mixed_store.start()
    other_piece = pieces.at[corner]
    remote(other_piece, other_piece, f_send.at[0], f_recv.at[5], on_chip).wait_recv()
    place_piece(corner)

    full, six = portion.at[pl.ds(0, count)], portion.at[pl.ds(0, count - 2)]
    for i, block in enumerate((full, six, full, six)):
        remote(block, block, d_send.at[i], first_recv.at[0], on_chip).wait_send()
    for i, block in enumerate((slots, slots, slots, back)):
        remote(block, block, c_send.at[i], slot_recv.at[0], on_chip).wait_send()
    for w in range(2):
        whole(w, 3).wait_send()
    both_edges().wait_send()
    three = pieces.at[pl.ds(0, 3)]
    remote(three, three, f_send.at[0], f_recv.at[5], on_chip).wait_send()
    mixed_store.wait()
    pltpu.make_async_copy(mixed, result_hbm, store.at[0]).wait()


FIRST_ORDER = (1, 4, 5, 2, 3, 6, 7)
ORDER = (1, 4, 5, 2, 6, 3, 7, 0)


def finish_kernel(mixed, result, mixed_out, result_out, held, into, out):
    step = held.shape[1] // 4
    loads, stores = [], []
    for i, source in enumerate((result, mixed)):
        for j in range(4):
            rows = pl.ds(step * j, step)
            copy = pltpu.make_async_copy(source.at[rows], held.at[i, rows], into.at[4 * i + j])
            copy.start()
            loads.append(copy)
    for i, target in enumerate((result_out, mixed_out)):
        for j in range(4):
            rows = pl.ds(step * j, step)
            loads[4 * i + j].wait()
            copy = pltpu.make_async_copy(held.at[i, rows], target.at[rows], out.at[4 * i + j])
            copy.start()
            stores.append(copy)
    for copy in stores:
        copy.wait()


def finish(mixed, result):
    anywhere = pl.BlockSpec(memory_space=pl.ANY)
    return pl.pallas_call(
        finish_kernel,
        out_shape=tuple(jax.ShapeDtypeStruct(x.shape, x.dtype) for x in (mixed, result)),
        in_specs=[anywhere] * 2,
        out_specs=(anywhere, anywhere),
        scratch_shapes=[
            pltpu.VMEM((2,) + result.shape, result.dtype),
            pltpu.SemaphoreType.DMA((8,)),
            pltpu.SemaphoreType.DMA((8,)),
        ],
        name="finish",
    )(mixed, result)


def fused(
    first_batch, mixer_gain, mixer_in, group_maps, pool_scale, mixer_out,
    second_batch, expert_gain, expert_choice, route_scores, expert_gate, expert_up, expert_down,
):
    rows, width = second_batch.shape
    count = lax.axis_size("ep")
    channels = pool_scale.shape[0]
    ff = expert_gate.shape[2]
    share = rows // count
    capacity = 4 * share
    quarter = width // 4
    tiles = ff // 128
    chunk = pltpu.VMEM((count, capacity, quarter), BF16)
    dma = pltpu.SemaphoreType.DMA
    in_hbm = pl.BlockSpec(memory_space=pltpu.HBM)
    operands = (
        first_batch, mixer_gain.reshape(1, width), mixer_in,
        group_maps.reshape(channels, GROUP), pool_scale.reshape(1, channels), mixer_out,
        second_batch, expert_gain.reshape(1, width), expert_choice.T, route_scores.T,
        expert_gate, expert_up, expert_down,
    )
    return finish(*pl.pallas_call(
        layer_kernel,
        out_shape=(
            jax.ShapeDtypeStruct(first_batch.shape, BF16),
            jax.ShapeDtypeStruct(second_batch.shape, BF16),
        ),
        in_specs=[in_hbm] * len(operands),
        out_specs=(in_hbm, in_hbm),
        scratch_shapes=[
            pltpu.VMEM((rows, width), BF16),
            pltpu.VMEM((rows, width), BF16),
            pltpu.VMEM((rows, width), BF16),
            pltpu.VMEM((rows, width), BF16),
            pltpu.VMEM((1, width), F32),
            pltpu.VMEM((1, width), F32),
            pltpu.VMEM((1, channels), F32),
            pltpu.VMEM((2, rows), jnp.int32),
            pltpu.VMEM((2, rows), F32),
            pltpu.VMEM((channels, GROUP), BF16),
            pltpu.VMEM((tiles, width, 256), BF16),
            pltpu.VMEM((ff, width), BF16),
            pltpu.VMEM((width, channels), BF16),
            pltpu.VMEM((channels, width), BF16),
            pltpu.VMEM((16, rows), F32),
            pltpu.VMEM((count * share + capacity, rows), BF16),
            pltpu.VMEM((count, share, width), BF16),
            pltpu.VMEM((count, 4, share, width), BF16),
            pltpu.VMEM((4 * capacity, ff), BF16),
            pltpu.VMEM((count, 4, capacity, quarter), BF16),
        ]
        + [chunk] * 6
        + [
            pltpu.VMEM((rows, count * capacity), BF16),
            pltpu.VMEM((rows, count * capacity), BF16),
            pltpu.VMEM((4, rows, quarter), BF16),
            pltpu.VMEM((rows + 32, channels), BF16),
            pltpu.VMEM((rows + 32, channels), F32),
            pltpu.VMEM((rows, channels), BF16),
            pltpu.VMEM((rows, width), BF16),
            dma((12,)),
            dma((4,)),
            dma((count,)),
            dma((count,)),
            dma((count // 2,)),
            dma((4,)),
            dma((count // 2,)),
            dma((count,)),
            dma((1,)),
            dma((2,)),
            dma((2, 4)),
            dma((1,)),
            dma((1,)),
            dma((1,)),
            dma((6,)),
            dma((2,)),
        ],
        compiler_params=pltpu.CompilerParams(
            collective_id=0, has_side_effects=True, vmem_limit_bytes=VMEM_LIMIT
        ),
        cost_estimate=pl.CostEstimate(flops=7 * 10**9, bytes_accessed=2**24, transcendentals=0),
        name="layer",
    )(*operands))


def per_device(*operands):
    if lax.axis_size("tp") == 4 and lax.axis_size("ep") == 8:
        return fused(*operands)
    return mixer_half(*operands[:6]), expert_half(*operands[6:])


def solution(mesh):
    placed = (
        P(("ep", "tp"), None),
        P(),
        P(None, "tp"),
        P(),
        P(),
        P("tp", None),
        P("ep", None),
        P(),
        P("ep", None),
        P("ep", None),
        P("ep", None, "tp"),
        P("ep", None, "tp"),
        P("ep", "tp", None),
    )
    return jax.shard_map(
        per_device,
        mesh=mesh,
        in_specs=placed,
        out_specs=(P(("ep", "tp"), None), P("ep", None)),
        check_vma=False,
    )
```

```python
import jax
import jax.numpy as jnp
from jax import lax
from jax.experimental import pallas as pl
from jax.experimental.pallas import tpu as pltpu
from jax.sharding import PartitionSpec as P

GROUP = 64
SEQS = 1


epsilon = 1e-06


def extended(block, sides, width):
    for axis, dim in sides:
        count = lax.axis_size(axis)
        forward = [(i, i + 1) for i in range(count - 1)]
        backward = [(target, source) for source, target in forward]
        low = lax.ppermute(
            lax.slice_in_dim(block, block.shape[dim] - width, None, axis=dim), axis, forward
        )
        high = lax.ppermute(lax.slice_in_dim(block, 0, width, axis=dim), axis, backward)
        block = jnp.concatenate([low, block, high], axis=dim)
    return block


def rms_scale(values, gain):
    floats = values.astype(jnp.float32)
    factor = lax.rsqrt(jnp.mean(floats * floats, axis=-1, keepdims=True) + epsilon)
    return (floats * factor * gain).astype(jnp.bfloat16)


def mixer_half(first_batch, mixer_gain, mixer_in, group_maps, pool_scale, mixer_out):
    count_rows = first_batch.shape[0]
    normed = rms_scale(first_batch, mixer_gain)
    pooled_in = jnp.dot(
        normed,
        lax.all_gather(mixer_in, "tp", axis=1, tiled=True),
        preferred_element_type=jnp.float32,
    ).astype(jnp.bfloat16)
    channels = pooled_in.shape[1]
    padded = extended(pooled_in, ((("ep", "tp"), 0),), 8).astype(jnp.float32)
    devices = lax.axis_size("ep") * lax.axis_size("tp")
    seq_length = count_rows * devices // SEQS
    first_row = (lax.axis_index("ep") * lax.axis_size("tp") + lax.axis_index("tp")) * count_rows
    places = first_row + jnp.arange(count_rows, dtype=jnp.int32)
    own_seq = places // seq_length
    group_of = jnp.arange(channels, dtype=jnp.int32) // GROUP
    half_span = jnp.left_shift(jnp.ones_like(group_of), group_of % 4)
    window_sum = jnp.zeros((count_rows, channels), jnp.float32)
    window_count = jnp.zeros((count_rows, channels), jnp.float32)
    for offset in range(-8, 8):
        inside = (
            ((places + offset) // seq_length == own_seq)[:, None]
            & (offset >= -half_span)[None, :]
            & (offset < half_span)[None, :]
        )
        window_sum = window_sum + jnp.where(
            inside, padded[8 + offset : 8 + offset + count_rows], 0.0
        )
        window_count = window_count + inside.astype(jnp.float32)
    centred = (window_sum / window_count - padded[8 : 8 + count_rows]).astype(jnp.bfloat16)
    group_count = group_maps.shape[0]
    identity = jnp.eye(group_count, dtype=jnp.bfloat16)
    block_map = jnp.einsum("gcd,gh->gchd", group_maps, identity).reshape(channels, channels)
    grouped = (jnp.dot(centred, block_map, preferred_element_type=jnp.float32) * pool_scale).astype(
        jnp.bfloat16
    )
    mixed_out = jnp.dot(
        grouped,
        lax.all_gather(mixer_out, "tp", axis=0, tiled=True),
        preferred_element_type=jnp.float32,
    )
    return mixed_out.astype(jnp.bfloat16)


def expert_half(
    second_batch, expert_gain, expert_choice, route_scores, expert_gate, expert_up, expert_down
):
    row_count = second_batch.shape[0]
    model_width = second_batch.shape[1]
    experts = lax.axis_size("ep")
    tp_count = lax.axis_size("tp")
    capacity = 4 * row_count // experts
    share = capacity // tp_count
    normed = rms_scale(second_batch, expert_gain)
    chosen = expert_choice.reshape(-1)
    one_hot = (chosen[:, None] == jnp.arange(experts, dtype=jnp.int32)[None, :]).astype(jnp.int32)
    ranking = jnp.sum(jnp.cumsum(one_hot, axis=0) * one_hot, axis=1) - 1
    slot_place = ranking * experts + chosen
    source_row = jnp.arange(chosen.shape[0], dtype=jnp.int32) // expert_choice.shape[1]
    slot_table = jnp.zeros((capacity * experts,), jnp.int32).at[slot_place].set(source_row + 1)
    outgoing = jnp.where(
        (slot_table > 0)[:, None],
        normed[jnp.maximum(slot_table - 1, 0)],
        jnp.zeros((), jnp.bfloat16),
    )
    outgoing = outgoing.reshape(capacity, experts, model_width)
    portion = lax.dynamic_slice_in_dim(outgoing, lax.axis_index("tp") * share, share, 0)
    arrived_part = lax.all_to_all(portion, "ep", split_axis=1, concat_axis=1, tiled=True)
    arrived = lax.all_gather(arrived_part, "tp", axis=0, tiled=True)
    incoming = arrived.reshape(capacity * experts, model_width)
    gate_weight = expert_gate[0]
    up_weight = expert_up[0]
    down_weight = expert_down[0]
    gate_part = jnp.dot(incoming, gate_weight, preferred_element_type=jnp.float32)
    up_part = jnp.dot(incoming, up_weight, preferred_element_type=jnp.float32)
    hidden = (jax.nn.silu(gate_part) * up_part).astype(jnp.bfloat16)
    summed = lax.psum_scatter(
        jnp.dot(hidden, down_weight, preferred_element_type=jnp.float32).astype(jnp.bfloat16),
        "tp",
        scatter_dimension=0,
        tiled=True,
    )
    finished = summed.reshape(share, experts, model_width)
    returned = lax.all_to_all(finished, "ep", split_axis=1, concat_axis=1, tiled=True)
    every_slot = lax.all_gather(returned, "tp", axis=0, tiled=True).reshape(
        capacity * experts, model_width
    )
    picked = every_slot[slot_place].reshape(row_count, -1, model_width)
    weight_first = jax.nn.sigmoid(route_scores[:, 0] - route_scores[:, 1])[:, None]
    blended = weight_first * picked[:, 0].astype(jnp.float32) + (1.0 - weight_first) * picked[
        :, 1
    ].astype(jnp.float32)
    return blended.astype(jnp.bfloat16)


MESH = pl.DeviceIdType.MESH
VMEM_LIMIT = 60 * 1024 * 1024
F32 = jnp.float32
BF16 = jnp.bfloat16


def flip(row, relation):
    place = row
    for bit in (1, 2, 4):
        if relation & bit:
            place = place + bit * (1 - 2 * ((row // bit) % 2))
    return place


def normalize(source, gain, target):
    for i in range(0, source.shape[0], 16):
        floats = source[i : i + 16].astype(F32)
        factor = lax.rsqrt(jnp.mean(floats * floats, axis=-1, keepdims=True) + epsilon)
        target[i : i + 16] = (floats * factor * gain[...]).astype(BF16)


def layer_kernel(
    first_hbm, mixer_gain_hbm, mixer_in_hbm, maps_hbm, scale_hbm, mixer_out_hbm,
    second_hbm, expert_gain_hbm, choice_hbm, scores_hbm, gate_hbm, up_hbm, down_hbm,
    mixed_hbm, result_hbm,
    x1, x2, n1, n2, gain1, gain2, scale, choice, scores, maps,
    w_in, w_down, m1, m2,
    rank_of, pick, portion, landed, hidden, part,
    side_y, side_own, sums_y, from_y, sums, slots, high, low, pieces,
    padded, floats, grouped, mixed,
    load, d_send, first_recv, y_recv, block_recv, c_send, part_recv, sum_recv, slot_recv,
    m_send, m_recv, h_send, h_recv, f_send, f_recv, store,
):
    row, col = lax.axis_index("ep"), lax.axis_index("tp")
    count = landed.shape[0]
    share = landed.shape[2]
    capacity = 4 * share
    rows, width = x2.shape
    quarter = width // 4
    tiles = w_in.shape[0]
    shard = m1.shape[1] // 4
    partner = col + 1 - 2 * (col % 2)
    across = (col + 2) % 4
    corner = (partner + 2) % 4
    devices = 4 * count
    index = row * 4 + col
    after, before = (index + 1) % devices, (index + devices - 1) % devices
    after_device, before_device = (after // 4, after % 4), (before // 4, before % 4)
    peer = [(flip(row, k), col) for k in range(count)]
    on_chip, over_y = (row, partner), (row, across)

    at = {k: i for i, k in enumerate(ORDER)}

    def remote(source, target, send, recv, device):
        return pltpu.make_async_remote_copy(
            src_ref=source, dst_ref=target, send_sem=send, recv_sem=recv,
            device_id=device, device_id_type=MESH,
        )

    def shard_of(which):
        return pl.ds(pl.multiple_of(which * shard, shard), shard)

    loads = {}

    def fetch(name, source, target):
        loads[name] = pltpu.make_async_copy(source, target, load.at[len(loads)])
        loads[name].start()

    fetch("x2", second_hbm, x2)
    fetch("gain2", expert_gain_hbm, gain2)
    fetch("choice", choice_hbm, choice)
    fetch("scores", scores_hbm, scores)
    fetch("m1", mixer_in_hbm, m1.at[:, shard_of(col)])
    fetch("m2", mixer_out_hbm, m2.at[shard_of(col)])
    fetch("x1", first_hbm, x1)
    fetch("gain1", mixer_gain_hbm, gain1)
    fetch("maps", maps_hbm, maps)
    fetch("scale", scale_hbm, scale)

    def fetch_weights():
        sem = load.at[len(loads)]
        for j in range(tiles):
            for i, source in enumerate((gate_hbm, up_hbm)):
                target = w_in.at[j, :, pl.ds(128 * i, 128)]
                pltpu.make_async_copy(source.at[0, :, pl.ds(128 * j, 128)], target, sem).start()
        loads["w_in"] = pltpu.make_async_copy(w_in, w_in, sem)
        fetch("down", down_hbm.at[0], w_down)

    barrier = pltpu.get_barrier_semaphore()
    peers = peer[1:] + [on_chip, over_y, after_device, before_device]
    for device in peers:
        pl.semaphore_signal(barrier, inc=1, device_id=device, device_id_type=MESH)

    loads["choice"].wait()
    experts = lax.broadcasted_iota(jnp.int32, (16, rows), 0)
    first, second = choice[0:1], choice[1:2]
    named = (first == experts) | (second == experts)
    earlier = lax.broadcasted_iota(jnp.int32, (rows, rows), 0) < lax.broadcasted_iota(
        jnp.int32, (rows, rows), 1
    )
    rank = jnp.dot(
        named.astype(F32).astype(BF16), earlier.astype(F32).astype(BF16), preferred_element_type=F32
    )
    rank_of[...] = jnp.where(named, rank, -1.0)

    def rank_at(k):
        return rank_of[pl.ds(peer[k][0], 1), :]

    place = lax.broadcasted_iota(jnp.int32, (capacity, rows), 0).astype(F32)
    core = col % 2
    offset = (col * share).astype(F32)
    for k in range(2, count):
        chosen = place[:share] + offset == rank_at(k)
        pick[(k - 2) * share : (k - 1) * share] = chosen.astype(F32).astype(BF16)
    far = (count - 2) * share
    pair = (core * 2 * share).astype(F32)
    chosen = place[: 2 * share] + pair == rank_at(1)
    pick[far : far + 2 * share] = chosen.astype(F32).astype(BF16)
    own = far + 2 * share
    pick[own:] = (place == rank_at(0)).astype(F32).astype(BF16)

    loads["x2"].wait()
    loads["gain2"].wait()
    normalize(x2, gain2, n2)
    for n in range(0, width, 256):
        taken = jnp.dot(pick[...], n2[:, n : n + 256], preferred_element_type=F32).astype(BF16)
        portion[:, :, n : n + 256] = taken[:own].reshape(count, share, 256)
        landed[at[0], :, :, n : n + 256] = taken[own:].reshape(4, share, 256)

    loads["m1"].wait()
    loads["m2"].wait()
    pl.semaphore_wait(barrier, len(peers))

    firsts, ys, sides, corners = {}, {}, {}, {}
    halves = landed.at[at[1], pl.ds(2 * core, 2)]
    for k in FIRST_ORDER:
        if k == 1:
            source, target = portion.at[pl.ds(count - 2, 2)], halves
        else:
            source, target = portion.at[k - 2], landed.at[at[k], col]
        firsts[k] = remote(source, target, d_send.at[0], first_recv.at[k], peer[k])
        firsts[k].start()

    def forward(k):
        firsts[k].wait_recv()
        if k == 1:
            sides[k] = remote(halves, halves, d_send.at[2], block_recv.at[at[k] // 2], on_chip)
            sides[k].start()
            return
        block = landed.at[at[k], col]
        ys[k] = remote(block, block, d_send.at[1], y_recv.at[k], over_y)
        ys[k].start()
        sides[k] = remote(block, block, d_send.at[2], block_recv.at[at[k] // 2], on_chip)
        sides[k].start()

    def turn(k):
        ys[k].wait_recv()
        block = landed.at[at[k], across]
        corners[k] = remote(block, block, d_send.at[3], block_recv.at[at[k] // 2], on_chip)
        corners[k].start()

    fourth = (row % 2) * 2 + (row // 2) % 2

    def piece(which, owner, start, size):
        if which == 0:
            unit = m1.shape[0] // 4
            return m1.at[pl.ds(pl.multiple_of(start * unit, unit), size * unit), shard_of(owner)]
        unit = shard // 4
        return m2.at[pl.ds(pl.multiple_of(owner * shard + start * unit, unit), size * unit)]

    def move(which, kind, owner, start, size, device):
        block = piece(which, owner, start, size)
        copy = remote(block, block, m_send.at[which], m_recv.at[which, kind], device)
        copy.start()
        return copy

    by_y, by_z, by_x = {}, {}, {}
    for w in range(2):
        by_y[w] = move(w, 0, col, fourth, 1, over_y)
    for w in range(2):
        move(w, 3, col, 0, 4, on_chip)

    def spread_z(w):
        by_y[w].wait_recv()
        by_z[w] = move(w, 1, across, fourth, 1, peer[2])
        move(w, 3, across, fourth, 1, on_chip)

    def spread_x(w):
        by_z[w].wait_recv()
        other = fourth + 1 - 2 * (fourth % 2)
        by_x[w] = move(w, 2, across, 2 * (fourth // 2), 2, peer[1])
        move(w, 3, across, other, 1, on_chip)

    def pass_on(w):
        by_x[w].wait_recv()
        move(w, 3, across, 2 - 2 * (fourth // 2), 2, on_chip)

    def whole(which, parts):
        ref = (m1, m2)[which]
        block = ref.at[pl.ds(0, ref.shape[0] * parts // 4)]
        return remote(block, block, m_send.at[which], m_recv.at[which, 3], on_chip)

    def gathered(w):
        whole(w, 2).wait_recv()

    def make_table():
        loads["scores"].wait()
        weight_first = jax.nn.sigmoid(scores[0:1] - scores[1:2])
        for k in range(0, count, 2):
            blocks = []
            for i in ORDER[k : k + 2]:
                weight = jnp.where(first == peer[i][0], weight_first, 1.0 - weight_first)
                blocks.append(jnp.where(place == rank_at(i), weight, 0.0))
            table = jnp.concatenate(blocks, axis=0).T
            top = table.astype(BF16)
            columns = slice(k * capacity, (k + 2) * capacity)
            high[:, columns] = top
            low[:, columns] = (table - top.astype(F32)).astype(BF16)

    def arrive(chunk):
        blocks = sum(2 for k in ORDER[2 * chunk : 2 * chunk + 2] if k)
        landing = landed.at[2 * chunk, pl.ds(0, blocks)]
        remote(landing, landing, d_send.at[2], block_recv.at[chunk], on_chip).wait_recv()

    weights_ready = set()

    def ready(name):
        if name not in weights_ready:
            weights_ready.add(name)
            loads[name].wait()

    to_side, to_own, to_y, to_ep = {}, {}, {}, {}

    def raise_up(start, stop, chosen):
        size = (stop - start) * capacity
        ready("w_in")
        for j in chosen:
            both = jnp.dot(
                landed[start:stop].reshape(size, width), w_in[j], preferred_element_type=F32
            )
            gate = both[:, :128]
            hidden[:size, 128 * j : 128 * j + 128] = (
                gate / (1.0 + jnp.exp(-gate)) * both[:, 128:]
            ).astype(BF16)

    def lower(start, stop, chosen):
        ready("down")
        size = (stop - start) * capacity
        for i in chosen:
            which = (corner, partner, across, col)[i]
            for h in range(0, quarter, 256):
                columns = pl.ds(pl.multiple_of(which * quarter + h, 256), 256)
                part[start:stop, i, :, h : h + 256] = (
                    jnp.dot(hidden[:size], w_down[:, columns], preferred_element_type=F32)
                    .astype(BF16)
                    .reshape(stop - start, capacity, 256)
                )

    def share_part(start, stop):
        for i, k in enumerate(ORDER[start:stop], start):
            to_side[k] = remote(
                part.at[i, 0], side_y.at[i], c_send.at[0], part_recv.at[i // 2], on_chip
            )
            to_side[k].start()
        for i, k in enumerate(ORDER[start:stop], start):
            to_own[k] = remote(
                part.at[i, 1], side_own.at[i], c_send.at[1], part_recv.at[i // 2], on_chip
            )
            to_own[k].start()

    def expert(start, stop, within=(), between=()):
        middle = tiles // 2 if within else 0
        raise_up(start, stop, range(middle))
        for step in within:
            step()
        raise_up(start, stop, range(middle, tiles))
        for step in between:
            step()
        lower(start, stop, (0, 1))
        share_part(start, stop)
        lower(start, stop, (2, 3))

    met = set()

    def halved(chunk):
        if chunk not in met:
            met.add(chunk)
            block = side_y.at[pl.ds(0, 4)]
            remote(block, block, c_send.at[0], part_recv.at[chunk], on_chip).wait_recv()

    def add_y(*ks):
        for k in ks:
            i = at[k]
            halved(i // 2)
            sums_y[i] = (part[i, 2].astype(F32) + side_y[i].astype(F32)).astype(BF16)
            to_y[k] = remote(sums_y.at[i], from_y.at[i], c_send.at[2], sum_recv.at[k], over_y)
            to_y[k].start()

    def add_all(*ks):
        for k in ks:
            i = at[k]
            to_y[k].wait_recv()
            total = (
                part[i, 3].astype(F32) + side_own[i].astype(F32) + from_y[i].astype(F32)
            ).astype(BF16)
            if k == 0:
                slots[i] = total
                continue
            sums[i] = total
            to_ep[k] = remote(sums.at[i], slots.at[i], c_send.at[3], slot_recv.at[0], peer[k])
            to_ep[k].start()

    halo = {}

    def mix_norm():
        loads["x1"].wait()
        loads["gain1"].wait()
        normalize(x1, gain1, n1)

    def mix_in():
        gathered(0)
        for n in range(0, m1.shape[1], 256):
            padded[16 : 16 + rows, n : n + 256] = jnp.dot(
                n1[...], m1[:, n : n + 256], preferred_element_type=F32
            ).astype(BF16)

    def mix_edges():
        halo[0] = remote(
            padded.at[pl.ds(rows, 16)], padded.at[pl.ds(0, 16)], h_send.at[0], h_recv.at[0],
            after_device,
        )
        halo[0].start()
        halo[1] = remote(
            padded.at[pl.ds(16, 16)], padded.at[pl.ds(16 + rows, 16)], h_send.at[0], h_recv.at[0],
            before_device,
        )
        halo[1].start()

    def both_edges():
        edges = padded.at[pl.ds(0, 32)]
        return remote(edges, edges, h_send.at[0], h_recv.at[0], after_device)

    def mix_centre():
        both_edges().wait_recv()
        loads["maps"].wait()
        loads["scale"].wait()
        seq_length = rows * devices // SEQS
        opening = (index * rows) % seq_length
        keep_low = (opening > 0).astype(F32)
        keep_high = (opening + rows < seq_length).astype(F32)
        floats[16 : 16 + rows] = padded[16 : 16 + rows].astype(F32)
        low_rows, high_rows = padded[:16].astype(F32), padded[16 + rows :].astype(F32)
        floats[:16] = jnp.where(keep_low > 0, low_rows, 0.0)
        floats[16 + rows :] = jnp.where(keep_high > 0, high_rows, 0.0)
        position = opening + lax.broadcasted_iota(jnp.int32, (rows, 128), 0)
        lane = lax.broadcasted_iota(jnp.int32, (rows, 128), 1)
        line = lax.broadcasted_iota(jnp.int32, (128, 128), 0)
        across_lane = lax.broadcasted_iota(jnp.int32, (128, 128), 1)
        copies = (
            lax.broadcasted_iota(jnp.int32, (GROUP, 128), 0)
            == lax.broadcasted_iota(jnp.int32, (GROUP, 128), 1) % GROUP
        ).astype(F32).astype(BF16)
        for b in range(padded.shape[1] // 128):
            columns = slice(128 * b, 128 * b + 128)

            def window(span):
                total = floats[16 - span : 16 - span + rows, columns]
                for step in range(-span + 1, span):
                    total = total + floats[16 + step : 16 + step + rows, columns]
                held = jnp.minimum(position + span, seq_length) - jnp.maximum(position - span, 0)
                return total / held.astype(F32)

            small = 1 if b % 2 == 0 else 4
            mean = jnp.where(lane < GROUP, window(small), window(2 * small))
            centred = (mean - floats[16 : 16 + rows, columns]).astype(BF16)
            spread = jnp.dot(maps[columns], copies, preferred_element_type=F32)
            block = jnp.where(line // GROUP == across_lane // GROUP, spread, 0.0).astype(BF16)
            grouped[:, columns] = (
                jnp.dot(centred, block, preferred_element_type=F32) * scale[:, columns]
            ).astype(BF16)

    def mix_out():
        gathered(1)
        for n in range(0, width, 256):
            mixed[:, n : n + 256] = jnp.dot(
                grouped[...], m2[:, n : n + 256], preferred_element_type=F32
            ).astype(BF16)

    fetch_weights()
    make_table()
    mix_norm()
    spread_z(0)
    forward(4)
    forward(2)
    forward(1)
    forward(3)
    spread_z(1)
    turn(4)
    forward(5)
    arrive(0)
    expert(0, 2, between=[lambda: forward(6), lambda: turn(2)])
    turn(3)
    forward(7)
    spread_x(0)
    turn(5)
    add_y(4, 1)
    arrive(1)
    expert(2, 4, between=[lambda: turn(6)])
    spread_x(1)
    arrive(2)
    expert(4, 6, [lambda: add_y(5, 2)], [lambda: turn(7), lambda: add_all(4)])
    arrive(3)
    expert(6, 8, [lambda: add_y(6)])
    add_all(5, 1)
    pass_on(0)
    add_y(7, 3, 0)
    add_all(6)
    mix_in()
    mix_edges()
    add_all(2)
    add_all(7)
    pass_on(1)
    add_all(3, 0)
    mix_centre()
    mix_out()
    mixed_store = pltpu.make_async_copy(mixed, mixed_hbm, store.at[1])
    mixed_store.start()

    back = slots.at[pl.ds(0, count - 1)]
    remote(back, back, c_send.at[3], slot_recv.at[0], on_chip).wait_recv()
    bits = rows // 4
    out_y = {}
    returned = slots[...].reshape(count * capacity, quarter)
    pieces[col] = (
        jnp.dot(high[...], returned, preferred_element_type=F32)
        + jnp.dot(low[...], returned, preferred_element_type=F32)
    ).astype(BF16)
    for h in range(4):
        block = pieces.at[col, pl.ds(h * bits, bits)]
        out_y[h] = remote(block, block, f_send.at[0], f_recv.at[h], over_y)
        out_y[h].start()
    own_piece = pieces.at[col]
    out_side = remote(own_piece, own_piece, f_send.at[0], f_recv.at[4], on_chip)
    out_side.start()

    def place_piece(which):
        columns = pl.ds(pl.multiple_of(which * quarter, quarter), quarter)
        pltpu.make_async_copy(pieces.at[which], result_hbm.at[:, columns], store.at[0]).start()

    place_piece(col)
    for h in range(4):
        out_y[h].wait_recv()
        block = pieces.at[across, pl.ds(h * bits, bits)]
        remote(block, block, f_send.at[0], f_recv.at[5], on_chip).start()
    place_piece(across)
    out_side.wait_recv()
    place_piece(partner)
    other_piece = pieces.at[corner]
    remote(other_piece, other_piece, f_send.at[0], f_recv.at[5], on_chip).wait_recv()
    place_piece(corner)

    full, six = portion.at[pl.ds(0, count)], portion.at[pl.ds(0, count - 2)]
    for i, block in enumerate((full, six, full, six)):
        remote(block, block, d_send.at[i], first_recv.at[0], on_chip).wait_send()
    for i, block in enumerate((slots, slots, slots, back)):
        remote(block, block, c_send.at[i], slot_recv.at[0], on_chip).wait_send()
    for w in range(2):
        whole(w, 3).wait_send()
    both_edges().wait_send()
    three = pieces.at[pl.ds(0, 3)]
    remote(three, three, f_send.at[0], f_recv.at[5], on_chip).wait_send()
    mixed_store.wait()
    pltpu.make_async_copy(mixed, result_hbm, store.at[0]).wait()


FIRST_ORDER = (1, 4, 5, 2, 3, 6, 7)
ORDER = (1, 4, 5, 2, 6, 3, 7, 0)


def finish_kernel(mixed, result, mixed_out, result_out, held, into, out):
    step = held.shape[1] // 4
    loads, stores = [], []
    for i, source in enumerate((result, mixed)):
        for j in range(4):
            rows = pl.ds(step * j, step)
            copy = pltpu.make_async_copy(source.at[rows], held.at[i, rows], into.at[4 * i + j])
            copy.start()
            loads.append(copy)
    for i, target in enumerate((result_out, mixed_out)):
        for j in range(4):
            rows = pl.ds(step * j, step)
            loads[4 * i + j].wait()
            copy = pltpu.make_async_copy(held.at[i, rows], target.at[rows], out.at[4 * i + j])
            copy.start()
            stores.append(copy)
    for copy in stores:
        copy.wait()


def finish(mixed, result):
    anywhere = pl.BlockSpec(memory_space=pl.ANY)
    return pl.pallas_call(
        finish_kernel,
        out_shape=tuple(jax.ShapeDtypeStruct(x.shape, x.dtype) for x in (mixed, result)),
        in_specs=[anywhere] * 2,
        out_specs=(anywhere, anywhere),
        scratch_shapes=[
            pltpu.VMEM((2,) + result.shape, result.dtype),
            pltpu.SemaphoreType.DMA((8,)),
            pltpu.SemaphoreType.DMA((8,)),
        ],
        name="finish",
    )(mixed, result)


def fused(
    first_batch, mixer_gain, mixer_in, group_maps, pool_scale, mixer_out,
    second_batch, expert_gain, expert_choice, route_scores, expert_gate, expert_up, expert_down,
):
    rows, width = second_batch.shape
    count = lax.axis_size("ep")
    channels = pool_scale.shape[0]
    ff = expert_gate.shape[2]
    share = rows // count
    capacity = 4 * share
    quarter = width // 4
    tiles = ff // 128
    chunk = pltpu.VMEM((count, capacity, quarter), BF16)
    dma = pltpu.SemaphoreType.DMA
    in_hbm = pl.BlockSpec(memory_space=pltpu.HBM)
    operands = (
        first_batch, mixer_gain.reshape(1, width), mixer_in,
        group_maps.reshape(channels, GROUP), pool_scale.reshape(1, channels), mixer_out,
        second_batch, expert_gain.reshape(1, width), expert_choice.T, route_scores.T,
        expert_gate, expert_up, expert_down,
    )
    return finish(*pl.pallas_call(
        layer_kernel,
        out_shape=(
            jax.ShapeDtypeStruct(first_batch.shape, BF16),
            jax.ShapeDtypeStruct(second_batch.shape, BF16),
        ),
        in_specs=[in_hbm] * len(operands),
        out_specs=(in_hbm, in_hbm),
        scratch_shapes=[
            pltpu.VMEM((rows, width), BF16),
            pltpu.VMEM((rows, width), BF16),
            pltpu.VMEM((rows, width), BF16),
            pltpu.VMEM((rows, width), BF16),
            pltpu.VMEM((1, width), F32),
            pltpu.VMEM((1, width), F32),
            pltpu.VMEM((1, channels), F32),
            pltpu.VMEM((2, rows), jnp.int32),
            pltpu.VMEM((2, rows), F32),
            pltpu.VMEM((channels, GROUP), BF16),
            pltpu.VMEM((tiles, width, 256), BF16),
            pltpu.VMEM((ff, width), BF16),
            pltpu.VMEM((width, channels), BF16),
            pltpu.VMEM((channels, width), BF16),
            pltpu.VMEM((16, rows), F32),
            pltpu.VMEM((count * share + capacity, rows), BF16),
            pltpu.VMEM((count, share, width), BF16),
            pltpu.VMEM((count, 4, share, width), BF16),
            pltpu.VMEM((4 * capacity, ff), BF16),
            pltpu.VMEM((count, 4, capacity, quarter), BF16),
        ]
        + [chunk] * 6
        + [
            pltpu.VMEM((rows, count * capacity), BF16),
            pltpu.VMEM((rows, count * capacity), BF16),
            pltpu.VMEM((4, rows, quarter), BF16),
            pltpu.VMEM((rows + 32, channels), BF16),
            pltpu.VMEM((rows + 32, channels), F32),
            pltpu.VMEM((rows, channels), BF16),
            pltpu.VMEM((rows, width), BF16),
            dma((12,)),
            dma((4,)),
            dma((count,)),
            dma((count,)),
            dma((count // 2,)),
            dma((4,)),
            dma((count // 2,)),
            dma((count,)),
            dma((1,)),
            dma((2,)),
            dma((2, 4)),
            dma((1,)),
            dma((1,)),
            dma((1,)),
            dma((6,)),
            dma((2,)),
        ],
        compiler_params=pltpu.CompilerParams(
            collective_id=0, has_side_effects=True, vmem_limit_bytes=VMEM_LIMIT
        ),
        cost_estimate=pl.CostEstimate(flops=7 * 10**9, bytes_accessed=2**24, transcendentals=0),
        name="layer",
    )(*operands))


def per_device(*operands):
    if lax.axis_size("tp") == 4 and lax.axis_size("ep") == 8:
        return fused(*operands)
    return mixer_half(*operands[:6]), expert_half(*operands[6:])


def solution(mesh):
    placed = (
        P(("ep", "tp"), None),
        P(),
        P(None, "tp"),
        P(),
        P(),
        P("tp", None),
        P("ep", None),
        P(),
        P("ep", None),
        P("ep", None),
        P("ep", None, "tp"),
        P("ep", None, "tp"),
        P("ep", "tp", None),
    )
    return jax.shard_map(
        per_device,
        mesh=mesh,
        in_specs=placed,
        out_specs=(P(("ep", "tp"), None), P("ep", None)),
        check_vma=False,
    )
```

```python
import jax
import jax.numpy as jnp
from jax import lax
from jax.experimental import pallas as pl
from jax.experimental.pallas import tpu as pltpu
from jax.sharding import PartitionSpec as P

GROUP = 64
SEQS = 1


epsilon = 1e-06


def extended(block, sides, width):
    for axis, dim in sides:
        count = lax.axis_size(axis)
        forward = [(i, i + 1) for i in range(count - 1)]
        backward = [(target, source) for source, target in forward]
        low = lax.ppermute(
            lax.slice_in_dim(block, block.shape[dim] - width, None, axis=dim), axis, forward
        )
        high = lax.ppermute(lax.slice_in_dim(block, 0, width, axis=dim), axis, backward)
        block = jnp.concatenate([low, block, high], axis=dim)
    return block


def rms_scale(values, gain):
    floats = values.astype(jnp.float32)
    factor = lax.rsqrt(jnp.mean(floats * floats, axis=-1, keepdims=True) + epsilon)
    return (floats * factor * gain).astype(jnp.bfloat16)


def mixer_half(first_batch, mixer_gain, mixer_in, group_maps, pool_scale, mixer_out):
    count_rows = first_batch.shape[0]
    normed = rms_scale(first_batch, mixer_gain)
    pooled_in = jnp.dot(
        normed,
        lax.all_gather(mixer_in, "tp", axis=1, tiled=True),
        preferred_element_type=jnp.float32,
    ).astype(jnp.bfloat16)
    channels = pooled_in.shape[1]
    padded = extended(pooled_in, ((("ep", "tp"), 0),), 8).astype(jnp.float32)
    devices = lax.axis_size("ep") * lax.axis_size("tp")
    seq_length = count_rows * devices // SEQS
    first_row = (lax.axis_index("ep") * lax.axis_size("tp") + lax.axis_index("tp")) * count_rows
    places = first_row + jnp.arange(count_rows, dtype=jnp.int32)
    own_seq = places // seq_length
    group_of = jnp.arange(channels, dtype=jnp.int32) // GROUP
    half_span = jnp.left_shift(jnp.ones_like(group_of), group_of % 4)
    window_sum = jnp.zeros((count_rows, channels), jnp.float32)
    window_count = jnp.zeros((count_rows, channels), jnp.float32)
    for offset in range(-8, 8):
        inside = (
            ((places + offset) // seq_length == own_seq)[:, None]
            & (offset >= -half_span)[None, :]
            & (offset < half_span)[None, :]
        )
        window_sum = window_sum + jnp.where(
            inside, padded[8 + offset : 8 + offset + count_rows], 0.0
        )
        window_count = window_count + inside.astype(jnp.float32)
    centred = (window_sum / window_count - padded[8 : 8 + count_rows]).astype(jnp.bfloat16)
    group_count = group_maps.shape[0]
    identity = jnp.eye(group_count, dtype=jnp.bfloat16)
    block_map = jnp.einsum("gcd,gh->gchd", group_maps, identity).reshape(channels, channels)
    grouped = (jnp.dot(centred, block_map, preferred_element_type=jnp.float32) * pool_scale).astype(
        jnp.bfloat16
    )
    mixed_out = jnp.dot(
        grouped,
        lax.all_gather(mixer_out, "tp", axis=0, tiled=True),
        preferred_element_type=jnp.float32,
    )
    return mixed_out.astype(jnp.bfloat16)


def expert_half(
    second_batch, expert_gain, expert_choice, route_scores, expert_gate, expert_up, expert_down
):
    row_count = second_batch.shape[0]
    model_width = second_batch.shape[1]
    experts = lax.axis_size("ep")
    tp_count = lax.axis_size("tp")
    capacity = 4 * row_count // experts
    share = capacity // tp_count
    normed = rms_scale(second_batch, expert_gain)
    chosen = expert_choice.reshape(-1)
    one_hot = (chosen[:, None] == jnp.arange(experts, dtype=jnp.int32)[None, :]).astype(jnp.int32)
    ranking = jnp.sum(jnp.cumsum(one_hot, axis=0) * one_hot, axis=1) - 1
    slot_place = ranking * experts + chosen
    source_row = jnp.arange(chosen.shape[0], dtype=jnp.int32) // expert_choice.shape[1]
    slot_table = jnp.zeros((capacity * experts,), jnp.int32).at[slot_place].set(source_row + 1)
    outgoing = jnp.where(
        (slot_table > 0)[:, None],
        normed[jnp.maximum(slot_table - 1, 0)],
        jnp.zeros((), jnp.bfloat16),
    )
    outgoing = outgoing.reshape(capacity, experts, model_width)
    portion = lax.dynamic_slice_in_dim(outgoing, lax.axis_index("tp") * share, share, 0)
    arrived_part = lax.all_to_all(portion, "ep", split_axis=1, concat_axis=1, tiled=True)
    arrived = lax.all_gather(arrived_part, "tp", axis=0, tiled=True)
    incoming = arrived.reshape(capacity * experts, model_width)
    gate_weight = expert_gate[0]
    up_weight = expert_up[0]
    down_weight = expert_down[0]
    gate_part = jnp.dot(incoming, gate_weight, preferred_element_type=jnp.float32)
    up_part = jnp.dot(incoming, up_weight, preferred_element_type=jnp.float32)
    hidden = (jax.nn.silu(gate_part) * up_part).astype(jnp.bfloat16)
    summed = lax.psum_scatter(
        jnp.dot(hidden, down_weight, preferred_element_type=jnp.float32).astype(jnp.bfloat16),
        "tp",
        scatter_dimension=0,
        tiled=True,
    )
    finished = summed.reshape(share, experts, model_width)
    returned = lax.all_to_all(finished, "ep", split_axis=1, concat_axis=1, tiled=True)
    every_slot = lax.all_gather(returned, "tp", axis=0, tiled=True).reshape(
        capacity * experts, model_width
    )
    picked = every_slot[slot_place].reshape(row_count, -1, model_width)
    weight_first = jax.nn.sigmoid(route_scores[:, 0] - route_scores[:, 1])[:, None]
    blended = weight_first * picked[:, 0].astype(jnp.float32) + (1.0 - weight_first) * picked[
        :, 1
    ].astype(jnp.float32)
    return blended.astype(jnp.bfloat16)


MESH = pl.DeviceIdType.MESH
VMEM_LIMIT = 60 * 1024 * 1024
F32 = jnp.float32
BF16 = jnp.bfloat16


def flip(row, relation):
    place = row
    for bit in (1, 2, 4):
        if relation & bit:
            place = place + bit * (1 - 2 * ((row // bit) % 2))
    return place


def normalize(source, gain, target):
    for i in range(0, source.shape[0], 16):
        floats = source[i : i + 16].astype(F32)
        factor = lax.rsqrt(jnp.mean(floats * floats, axis=-1, keepdims=True) + epsilon)
        target[i : i + 16] = (floats * factor * gain[...]).astype(BF16)


def layer_kernel(
    first_hbm, mixer_gain_hbm, mixer_in_hbm, maps_hbm, scale_hbm, mixer_out_hbm,
    second_hbm, expert_gain_hbm, choice_hbm, scores_hbm, gate_hbm, up_hbm, down_hbm,
    mixed_hbm, result_hbm,
    x1, x2, n1, n2, gain1, gain2, scale, choice, scores, maps,
    w_in, w_down, m1, m2,
    rank_of, pick, portion, landed, hidden, part,
    side_y, side_own, sums_y, from_y, sums, slots, high, low, pieces,
    padded, floats, grouped, mixed,
    load, d_send, first_recv, y_recv, block_recv, c_send, part_recv, sum_recv, slot_recv,
    m_send, m_recv, h_send, h_recv, f_send, f_recv, store,
):
    row, col = lax.axis_index("ep"), lax.axis_index("tp")
    count = landed.shape[0]
    share = landed.shape[2]
    capacity = 4 * share
    rows, width = x2.shape
    quarter = width // 4
    tiles = w_in.shape[0]
    shard = m1.shape[1] // 4
    partner = col + 1 - 2 * (col % 2)
    across = (col + 2) % 4
    corner = (partner + 2) % 4
    devices = 4 * count
    index = row * 4 + col
    after, before = (index + 1) % devices, (index + devices - 1) % devices
    after_device, before_device = (after // 4, after % 4), (before // 4, before % 4)
    peer = [(flip(row, k), col) for k in range(count)]
    on_chip, over_y = (row, partner), (row, across)

    at = {k: i for i, k in enumerate(ORDER)}

    def remote(source, target, send, recv, device):
        return pltpu.make_async_remote_copy(
            src_ref=source, dst_ref=target, send_sem=send, recv_sem=recv,
            device_id=device, device_id_type=MESH,
        )

    def shard_of(which):
        return pl.ds(pl.multiple_of(which * shard, shard), shard)

    loads = {}

    def fetch(name, source, target):
        loads[name] = pltpu.make_async_copy(source, target, load.at[len(loads)])
        loads[name].start()

    fetch("x2", second_hbm, x2)
    fetch("gain2", expert_gain_hbm, gain2)
    fetch("choice", choice_hbm, choice)
    fetch("scores", scores_hbm, scores)
    fetch("m1", mixer_in_hbm, m1.at[:, shard_of(col)])
    fetch("m2", mixer_out_hbm, m2.at[shard_of(col)])
    fetch("x1", first_hbm, x1)
    fetch("gain1", mixer_gain_hbm, gain1)
    fetch("maps", maps_hbm, maps)
    fetch("scale", scale_hbm, scale)

    def fetch_weights():
        sem = load.at[len(loads)]
        for j in range(tiles):
            for i, source in enumerate((gate_hbm, up_hbm)):
                target = w_in.at[j, :, pl.ds(128 * i, 128)]
                pltpu.make_async_copy(source.at[0, :, pl.ds(128 * j, 128)], target, sem).start()
        loads["w_in"] = pltpu.make_async_copy(w_in, w_in, sem)
        fetch("down", down_hbm.at[0], w_down)

    barrier = pltpu.get_barrier_semaphore()
    peers = peer[1:] + [on_chip, over_y, after_device, before_device]
    for device in peers:
        pl.semaphore_signal(barrier, inc=1, device_id=device, device_id_type=MESH)

    loads["choice"].wait()
    experts = lax.broadcasted_iota(jnp.int32, (16, rows), 0)
    first, second = choice[0:1], choice[1:2]
    named = (first == experts) | (second == experts)
    earlier = lax.broadcasted_iota(jnp.int32, (rows, rows), 0) < lax.broadcasted_iota(
        jnp.int32, (rows, rows), 1
    )
    rank = jnp.dot(
        named.astype(F32).astype(BF16), earlier.astype(F32).astype(BF16), preferred_element_type=F32
    )
    rank_of[...] = jnp.where(named, rank, -1.0)

    def rank_at(k):
        return rank_of[pl.ds(peer[k][0], 1), :]

    place = lax.broadcasted_iota(jnp.int32, (capacity, rows), 0).astype(F32)
    core = col % 2
    offset = (col * share).astype(F32)
    for k in range(2, count):
        chosen = place[:share] + offset == rank_at(k)
        pick[(k - 2) * share : (k - 1) * share] = chosen.astype(F32).astype(BF16)
    far = (count - 2) * share
    pair = (core * 2 * share).astype(F32)
    chosen = place[: 2 * share] + pair == rank_at(1)
    pick[far : far + 2 * share] = chosen.astype(F32).astype(BF16)
    own = far + 2 * share
    pick[own:] = (place == rank_at(0)).astype(F32).astype(BF16)

    loads["x2"].wait()
    loads["gain2"].wait()
    normalize(x2, gain2, n2)
    for n in range(0, width, 256):
        taken = jnp.dot(pick[...], n2[:, n : n + 256], preferred_element_type=F32).astype(BF16)
        portion[:, :, n : n + 256] = taken[:own].reshape(count, share, 256)
        landed[at[0], :, :, n : n + 256] = taken[own:].reshape(4, share, 256)

    loads["m1"].wait()
    loads["m2"].wait()
    pl.semaphore_wait(barrier, len(peers))

    firsts, ys, sides, corners = {}, {}, {}, {}
    halves = landed.at[at[1], pl.ds(2 * core, 2)]
    for k in FIRST_ORDER:
        if k == 1:
            source, target = portion.at[pl.ds(count - 2, 2)], halves
        else:
            source, target = portion.at[k - 2], landed.at[at[k], col]
        firsts[k] = remote(source, target, d_send.at[0], first_recv.at[k], peer[k])
        firsts[k].start()

    def forward(k):
        firsts[k].wait_recv()
        if k == 1:
            sides[k] = remote(halves, halves, d_send.at[2], block_recv.at[at[k] // 2], on_chip)
            sides[k].start()
            return
        block = landed.at[at[k], col]
        ys[k] = remote(block, block, d_send.at[1], y_recv.at[k], over_y)
        ys[k].start()
        sides[k] = remote(block, block, d_send.at[2], block_recv.at[at[k] // 2], on_chip)
        sides[k].start()

    def turn(k):
        ys[k].wait_recv()
        block = landed.at[at[k], across]
        corners[k] = remote(block, block, d_send.at[3], block_recv.at[at[k] // 2], on_chip)
        corners[k].start()

    fourth = (row % 2) * 2 + (row // 2) % 2

    def piece(which, owner, start, size):
        if which == 0:
            unit = m1.shape[0] // 4
            return m1.at[pl.ds(pl.multiple_of(start * unit, unit), size * unit), shard_of(owner)]
        unit = shard // 4
        return m2.at[pl.ds(pl.multiple_of(owner * shard + start * unit, unit), size * unit)]

    def move(which, kind, owner, start, size, device):
        block = piece(which, owner, start, size)
        copy = remote(block, block, m_send.at[which], m_recv.at[which, kind], device)
        copy.start()
        return copy

    by_y, by_z, by_x = {}, {}, {}
    for w in range(2):
        by_y[w] = move(w, 0, col, fourth, 1, over_y)
    for w in range(2):
        move(w, 3, col, 0, 4, on_chip)

    def spread_z(w):
        by_y[w].wait_recv()
        by_z[w] = move(w, 1, across, fourth, 1, peer[2])
        move(w, 3, across, fourth, 1, on_chip)

    def spread_x(w):
        by_z[w].wait_recv()
        other = fourth + 1 - 2 * (fourth % 2)
        by_x[w] = move(w, 2, across, 2 * (fourth // 2), 2, peer[1])
        move(w, 3, across, other, 1, on_chip)

    def pass_on(w):
        by_x[w].wait_recv()
        move(w, 3, across, 2 - 2 * (fourth // 2), 2, on_chip)

    def whole(which, parts):
        ref = (m1, m2)[which]
        block = ref.at[pl.ds(0, ref.shape[0] * parts // 4)]
        return remote(block, block, m_send.at[which], m_recv.at[which, 3], on_chip)

    def gathered(w):
        whole(w, 2).wait_recv()

    def make_table():
        loads["scores"].wait()
        weight_first = jax.nn.sigmoid(scores[0:1] - scores[1:2])
        for k in range(0, count, 2):
            blocks = []
            for i in ORDER[k : k + 2]:
                weight = jnp.where(first == peer[i][0], weight_first, 1.0 - weight_first)
                blocks.append(jnp.where(place == rank_at(i), weight, 0.0))
            table = jnp.concatenate(blocks, axis=0).T
            top = table.astype(BF16)
            columns = slice(k * capacity, (k + 2) * capacity)
            high[:, columns] = top
            low[:, columns] = (table - top.astype(F32)).astype(BF16)

    def arrive(chunk):
        blocks = sum(2 for k in ORDER[2 * chunk : 2 * chunk + 2] if k)
        landing = landed.at[2 * chunk, pl.ds(0, blocks)]
        remote(landing, landing, d_send.at[2], block_recv.at[chunk], on_chip).wait_recv()

    weights_ready = set()

    def ready(name):
        if name not in weights_ready:
            weights_ready.add(name)
            loads[name].wait()

    to_side, to_own, to_y, to_ep = {}, {}, {}, {}

    def raise_up(start, stop, chosen):
        size = (stop - start) * capacity
        ready("w_in")
        for j in chosen:
            both = jnp.dot(
                landed[start:stop].reshape(size, width), w_in[j], preferred_element_type=F32
            )
            gate = both[:, :128]
            hidden[:size, 128 * j : 128 * j + 128] = (
                gate / (1.0 + jnp.exp(-gate)) * both[:, 128:]
            ).astype(BF16)

    def lower(start, stop, chosen):
        ready("down")
        size = (stop - start) * capacity
        for i in chosen:
            which = (corner, partner, across, col)[i]
            for h in range(0, quarter, 256):
                columns = pl.ds(pl.multiple_of(which * quarter + h, 256), 256)
                part[start:stop, i, :, h : h + 256] = (
                    jnp.dot(hidden[:size], w_down[:, columns], preferred_element_type=F32)
                    .astype(BF16)
                    .reshape(stop - start, capacity, 256)
                )

    def share_part(start, stop):
        for i, k in enumerate(ORDER[start:stop], start):
            to_side[k] = remote(
                part.at[i, 0], side_y.at[i], c_send.at[0], part_recv.at[i // 2], on_chip
            )
            to_side[k].start()
        for i, k in enumerate(ORDER[start:stop], start):
            to_own[k] = remote(
                part.at[i, 1], side_own.at[i], c_send.at[1], part_recv.at[i // 2], on_chip
            )
            to_own[k].start()

    def expert(start, stop, within=(), between=()):
        middle = tiles // 2 if within else 0
        raise_up(start, stop, range(middle))
        for step in within:
            step()
        raise_up(start, stop, range(middle, tiles))
        for step in between:
            step()
        lower(start, stop, (0, 1))
        share_part(start, stop)
        lower(start, stop, (2, 3))

    met = set()

    def halved(chunk):
        if chunk not in met:
            met.add(chunk)
            block = side_y.at[pl.ds(0, 4)]
            remote(block, block, c_send.at[0], part_recv.at[chunk], on_chip).wait_recv()

    def add_y(*ks):
        for k in ks:
            i = at[k]
            halved(i // 2)
            sums_y[i] = (part[i, 2].astype(F32) + side_y[i].astype(F32)).astype(BF16)
            to_y[k] = remote(sums_y.at[i], from_y.at[i], c_send.at[2], sum_recv.at[k], over_y)
            to_y[k].start()

    def add_all(*ks):
        for k in ks:
            i = at[k]
            to_y[k].wait_recv()
            total = (
                part[i, 3].astype(F32) + side_own[i].astype(F32) + from_y[i].astype(F32)
            ).astype(BF16)
            if k == 0:
                slots[i] = total
                continue
            sums[i] = total
            to_ep[k] = remote(sums.at[i], slots.at[i], c_send.at[3], slot_recv.at[0], peer[k])
            to_ep[k].start()

    halo = {}

    def mix_norm():
        loads["x1"].wait()
        loads["gain1"].wait()
        normalize(x1, gain1, n1)

    def mix_in():
        gathered(0)
        for n in range(0, m1.shape[1], 256):
            padded[16 : 16 + rows, n : n + 256] = jnp.dot(
                n1[...], m1[:, n : n + 256], preferred_element_type=F32
            ).astype(BF16)

    def mix_edges():
        halo[0] = remote(
            padded.at[pl.ds(rows, 16)], padded.at[pl.ds(0, 16)], h_send.at[0], h_recv.at[0],
            after_device,
        )
        halo[0].start()
        halo[1] = remote(
            padded.at[pl.ds(16, 16)], padded.at[pl.ds(16 + rows, 16)], h_send.at[0], h_recv.at[0],
            before_device,
        )
        halo[1].start()

    def both_edges():
        edges = padded.at[pl.ds(0, 32)]
        return remote(edges, edges, h_send.at[0], h_recv.at[0], after_device)

    def mix_centre():
        both_edges().wait_recv()
        loads["maps"].wait()
        loads["scale"].wait()
        seq_length = rows * devices // SEQS
        opening = (index * rows) % seq_length
        keep_low = (opening > 0).astype(F32)
        keep_high = (opening + rows < seq_length).astype(F32)
        floats[16 : 16 + rows] = padded[16 : 16 + rows].astype(F32)
        low_rows, high_rows = padded[:16].astype(F32), padded[16 + rows :].astype(F32)
        floats[:16] = jnp.where(keep_low > 0, low_rows, 0.0)
        floats[16 + rows :] = jnp.where(keep_high > 0, high_rows, 0.0)
        position = opening + lax.broadcasted_iota(jnp.int32, (rows, 128), 0)
        lane = lax.broadcasted_iota(jnp.int32, (rows, 128), 1)
        line = lax.broadcasted_iota(jnp.int32, (128, 128), 0)
        across_lane = lax.broadcasted_iota(jnp.int32, (128, 128), 1)
        copies = (
            lax.broadcasted_iota(jnp.int32, (GROUP, 128), 0)
            == lax.broadcasted_iota(jnp.int32, (GROUP, 128), 1) % GROUP
        ).astype(F32).astype(BF16)
        for b in range(padded.shape[1] // 128):
            columns = slice(128 * b, 128 * b + 128)

            def window(span):
                total = floats[16 - span : 16 - span + rows, columns]
                for step in range(-span + 1, span):
                    total = total + floats[16 + step : 16 + step + rows, columns]
                held = jnp.minimum(position + span, seq_length) - jnp.maximum(position - span, 0)
                return total / held.astype(F32)

            small = 1 if b % 2 == 0 else 4
            mean = jnp.where(lane < GROUP, window(small), window(2 * small))
            centred = (mean - floats[16 : 16 + rows, columns]).astype(BF16)
            spread = jnp.dot(maps[columns], copies, preferred_element_type=F32)
            block = jnp.where(line // GROUP == across_lane // GROUP, spread, 0.0).astype(BF16)
            grouped[:, columns] = (
                jnp.dot(centred, block, preferred_element_type=F32) * scale[:, columns]
            ).astype(BF16)

    def mix_out():
        gathered(1)
        for n in range(0, width, 256):
            mixed[:, n : n + 256] = jnp.dot(
                grouped[...], m2[:, n : n + 256], preferred_element_type=F32
            ).astype(BF16)

    fetch_weights()
    make_table()
    mix_norm()
    spread_z(0)
    forward(4)
    forward(2)
    forward(1)
    forward(3)
    spread_z(1)
    turn(4)
    forward(5)
    arrive(0)
    expert(0, 2, between=[lambda: forward(6), lambda: turn(2)])
    turn(3)
    forward(7)
    spread_x(0)
    turn(5)
    add_y(4, 1)
    arrive(1)
    expert(2, 4, between=[lambda: turn(6)])
    spread_x(1)
    arrive(2)
    expert(4, 6, [lambda: add_y(5), lambda: add_all(4)], [lambda: turn(7), lambda: add_y(2)])
    arrive(3)
    expert(6, 8, [lambda: add_y(6)])
    add_all(5, 1)
    pass_on(0)
    add_y(7, 3, 0)
    add_all(6)
    mix_in()
    mix_edges()
    add_all(2)
    add_all(7)
    pass_on(1)
    add_all(3, 0)
    mix_centre()
    mix_out()
    mixed_store = pltpu.make_async_copy(mixed, mixed_hbm, store.at[1])
    mixed_store.start()

    back = slots.at[pl.ds(0, count - 1)]
    remote(back, back, c_send.at[3], slot_recv.at[0], on_chip).wait_recv()
    bits = rows // 4
    out_y = {}
    returned = slots[...].reshape(count * capacity, quarter)
    pieces[col] = (
        jnp.dot(high[...], returned, preferred_element_type=F32)
        + jnp.dot(low[...], returned, preferred_element_type=F32)
    ).astype(BF16)
    for h in range(4):
        block = pieces.at[col, pl.ds(h * bits, bits)]
        out_y[h] = remote(block, block, f_send.at[0], f_recv.at[h], over_y)
        out_y[h].start()
    own_piece = pieces.at[col]
    out_side = remote(own_piece, own_piece, f_send.at[0], f_recv.at[4], on_chip)
    out_side.start()

    def place_piece(which):
        columns = pl.ds(pl.multiple_of(which * quarter, quarter), quarter)
        pltpu.make_async_copy(pieces.at[which], result_hbm.at[:, columns], store.at[0]).start()

    place_piece(col)
    for h in range(4):
        out_y[h].wait_recv()
        block = pieces.at[across, pl.ds(h * bits, bits)]
        remote(block, block, f_send.at[0], f_recv.at[5], on_chip).start()
    place_piece(across)
    out_side.wait_recv()
    place_piece(partner)
    other_piece = pieces.at[corner]
    remote(other_piece, other_piece, f_send.at[0], f_recv.at[5], on_chip).wait_recv()
    place_piece(corner)

    full, six = portion.at[pl.ds(0, count)], portion.at[pl.ds(0, count - 2)]
    for i, block in enumerate((full, six, full, six)):
        remote(block, block, d_send.at[i], first_recv.at[0], on_chip).wait_send()
    for i, block in enumerate((slots, slots, slots, back)):
        remote(block, block, c_send.at[i], slot_recv.at[0], on_chip).wait_send()
    for w in range(2):
        whole(w, 3).wait_send()
    both_edges().wait_send()
    three = pieces.at[pl.ds(0, 3)]
    remote(three, three, f_send.at[0], f_recv.at[5], on_chip).wait_send()
    mixed_store.wait()
    pltpu.make_async_copy(mixed, result_hbm, store.at[0]).wait()


FIRST_ORDER = (1, 4, 5, 2, 3, 6, 7)
ORDER = (1, 4, 5, 2, 6, 3, 7, 0)


def finish_kernel(mixed, result, mixed_out, result_out, held, into, out):
    step = held.shape[1]
    loads, stores = [], []
    for i, source in enumerate((result, mixed)):
        for j in range(1):
            rows = pl.ds(step * j, step)
            copy = pltpu.make_async_copy(source.at[rows], held.at[i, rows], into.at[i + j])
            copy.start()
            loads.append(copy)
    for i, target in enumerate((result_out, mixed_out)):
        for j in range(1):
            rows = pl.ds(step * j, step)
            loads[i + j].wait()
            copy = pltpu.make_async_copy(held.at[i, rows], target.at[rows], out.at[i + j])
            copy.start()
            stores.append(copy)
    for copy in stores:
        copy.wait()


def finish(mixed, result):
    anywhere = pl.BlockSpec(memory_space=pl.ANY)
    return pl.pallas_call(
        finish_kernel,
        out_shape=tuple(jax.ShapeDtypeStruct(x.shape, x.dtype) for x in (mixed, result)),
        in_specs=[anywhere] * 2,
        out_specs=(anywhere, anywhere),
        scratch_shapes=[
            pltpu.VMEM((2,) + result.shape, result.dtype),
            pltpu.SemaphoreType.DMA((2,)),
            pltpu.SemaphoreType.DMA((2,)),
        ],
        name="finish",
    )(mixed, result)


def fused(
    first_batch, mixer_gain, mixer_in, group_maps, pool_scale, mixer_out,
    second_batch, expert_gain, expert_choice, route_scores, expert_gate, expert_up, expert_down,
):
    rows, width = second_batch.shape
    count = lax.axis_size("ep")
    channels = pool_scale.shape[0]
    ff = expert_gate.shape[2]
    share = rows // count
    capacity = 4 * share
    quarter = width // 4
    tiles = ff // 128
    chunk = pltpu.VMEM((count, capacity, quarter), BF16)
    dma = pltpu.SemaphoreType.DMA
    in_hbm = pl.BlockSpec(memory_space=pltpu.HBM)
    operands = (
        first_batch, mixer_gain.reshape(1, width), mixer_in,
        group_maps.reshape(channels, GROUP), pool_scale.reshape(1, channels), mixer_out,
        second_batch, expert_gain.reshape(1, width), expert_choice.T, route_scores.T,
        expert_gate, expert_up, expert_down,
    )
    return finish(*pl.pallas_call(
        layer_kernel,
        out_shape=(
            jax.ShapeDtypeStruct(first_batch.shape, BF16),
            jax.ShapeDtypeStruct(second_batch.shape, BF16),
        ),
        in_specs=[in_hbm] * len(operands),
        out_specs=(in_hbm, in_hbm),
        scratch_shapes=[
            pltpu.VMEM((rows, width), BF16),
            pltpu.VMEM((rows, width), BF16),
            pltpu.VMEM((rows, width), BF16),
            pltpu.VMEM((rows, width), BF16),
            pltpu.VMEM((1, width), F32),
            pltpu.VMEM((1, width), F32),
            pltpu.VMEM((1, channels), F32),
            pltpu.VMEM((2, rows), jnp.int32),
            pltpu.VMEM((2, rows), F32),
            pltpu.VMEM((channels, GROUP), BF16),
            pltpu.VMEM((tiles, width, 256), BF16),
            pltpu.VMEM((ff, width), BF16),
            pltpu.VMEM((width, channels), BF16),
            pltpu.VMEM((channels, width), BF16),
            pltpu.VMEM((16, rows), F32),
            pltpu.VMEM((count * share + capacity, rows), BF16),
            pltpu.VMEM((count, share, width), BF16),
            pltpu.VMEM((count, 4, share, width), BF16),
            pltpu.VMEM((4 * capacity, ff), BF16),
            pltpu.VMEM((count, 4, capacity, quarter), BF16),
        ]
        + [chunk] * 6
        + [
            pltpu.VMEM((rows, count * capacity), BF16),
            pltpu.VMEM((rows, count * capacity), BF16),
            pltpu.VMEM((4, rows, quarter), BF16),
            pltpu.VMEM((rows + 32, channels), BF16),
            pltpu.VMEM((rows + 32, channels), F32),
            pltpu.VMEM((rows, channels), BF16),
            pltpu.VMEM((rows, width), BF16),
            dma((12,)),
            dma((4,)),
            dma((count,)),
            dma((count,)),
            dma((count // 2,)),
            dma((4,)),
            dma((count // 2,)),
            dma((count,)),
            dma((1,)),
            dma((2,)),
            dma((2, 4)),
            dma((1,)),
            dma((1,)),
            dma((1,)),
            dma((6,)),
            dma((2,)),
        ],
        compiler_params=pltpu.CompilerParams(
            collective_id=0, has_side_effects=True, vmem_limit_bytes=VMEM_LIMIT
        ),
        cost_estimate=pl.CostEstimate(flops=7 * 10**9, bytes_accessed=2**24, transcendentals=0),
        name="layer",
    )(*operands))


def per_device(*operands):
    if lax.axis_size("tp") == 4 and lax.axis_size("ep") == 8:
        return fused(*operands)
    return mixer_half(*operands[:6]), expert_half(*operands[6:])


def solution(mesh):
    placed = (
        P(("ep", "tp"), None),
        P(),
        P(None, "tp"),
        P(),
        P(),
        P("tp", None),
        P("ep", None),
        P(),
        P("ep", None),
        P("ep", None),
        P("ep", None, "tp"),
        P("ep", None, "tp"),
        P("ep", "tp", None),
    )
    return jax.shard_map(
        per_device,
        mesh=mesh,
        in_specs=placed,
        out_specs=(P(("ep", "tp"), None), P("ep", None)),
        check_vma=False,
    )
```
